32 devices in a mesh: ep: 8 (over z, y), tp: 4 (over x, core).
Axes of the slice: x: 2, y: 2, z: 4, core: 2. Of those that a mesh axis runs over, the one named last changes fastest.
Arguments:
- tokens: bfloat16 [256, 2048], P('ep'), may hold values from -6 to 6
- kv_cache: bfloat16 [256, 1024, 512], P('ep', None, 'tp'), may hold values from -320 to 320
- lengths: int32 [256], P('ep'), may hold values from 1 to 1024, 131072 in all
- attn_gain: float32 [2048], replicated, may hold values from 0.1 to 1.9
- w_query: bfloat16 [2048, 1024], P(None, 'tp'), may hold values from -0.125 to 0.125
- w_key: bfloat16 [2048, 256], P(None, 'tp'), may hold values from -0.125 to 0.125
- w_value: bfloat16 [2048, 256], P(None, 'tp'), may hold values from -0.125 to 0.125
- lambdas: float32 [16], P('tp'), may hold values from 0.3 to 0.8
- head_gain: float32 [64], replicated, may hold values from 0.1 to 1.9
- w_out: bfloat16 [1024, 2048], replicated, may hold values from -0.1875 to 0.1875
- ffn_gain: float32 [2048], replicated, may hold values from 0.1 to 1.9
- w_shared_gate: bfloat16 [2048, 512], P(None, 'tp'), may hold values from -0.125 to 0.125
- w_shared_up: bfloat16 [2048, 512], P(None, 'tp'), may hold values from -0.125 to 0.125
- w_shared_down: bfloat16 [512, 2048], P('tp'), may hold values from -0.25 to 0.25
- routing: int32 [256, 4], replicated, may hold values from 0 to 31, all different within a row; in each aligned block of 32 rows (0 to 31, 32 to 63, ...) at most 8 rows name the same one
- route_weights: float32 [256, 4], P('ep'), may hold values from 0.1 to 1
- w_exp_gate: bfloat16 [32, 2048, 512], P(('ep', 'tp')), may hold values from -0.125 to 0.125
- w_exp_up: bfloat16 [32, 2048, 512], P(('ep', 'tp')), may hold values from -0.125 to 0.125
- w_exp_down: bfloat16 [32, 512, 2048], P(('ep', 'tp')), may hold values from -0.25 to 0.25
Outputs:
- mixed: bfloat16 [256, 2048], P('ep', 'tp')
The draws below stay inside these ranges and needn't reach their ends.
Inputs may be any that keep to these rules, and one draw needn't show every extreme that they name: `lengths`: A sequence's cache holds its past keys and values at positions below its length, and the new token follows them; some sequence uses all 1024 positions. `routing`: each row names 4 different experts. Within the rows of one group of 32 sequences (aligned blocks) no expert is named by more than 8 rows, and in some blocks an expert is named by exactly 8.
All inputs are finite; a program needn't handle non-finite values. No bound on the sum of `lengths` on one device may be relied on, other than what follows from the above.
Results may differ from the reference program's by a relative error of at most 0.015.
The reference program's roundings to bfloat16 on the way count: a program that leaves them out, or rounds other values in their place, can miss the bound.
Values may be sent and summed in bfloat16 or wider, within the bound.
A program may use at most 128 MiB of HBM per device.

```python
import math
import jax
import jax.numpy as jnp
import numpy as np
from jax import lax

D = 2048
HEADS = 16
KV_HEADS = 4
QK_DIM = 32
V_DIM = 64
FF_S = 512
FF_E = 512
TOPK = 4
SEQ_DEV = 32
CACHE = 1024
BATCH = 256
EXPERTS = 32
CAP = 8
N_EP = 8
N_TP = 4


def draw_kv_cache(key, part):
    key_base = jax.random.fold_in(key, 0)
    full_shape = (BATCH, CACHE, KV_HEADS, 2, 2 * QK_DIM)
    base_draw = jax.random.normal(key_base, full_shape, jnp.float32)
    scales = jnp.array([1.75, 1.0], jnp.float32)
    entries = base_draw * scales[:, None]
    return entries.reshape(BATCH, CACHE, KV_HEADS * 4 * QK_DIM).astype(jnp.bfloat16)


def steps_of(key, dims, cuts, smallest, top_value):
    loudness = 1.0
    for dim, blocks in cuts:
        draws = jax.random.uniform(jax.random.fold_in(jax.random.fold_in(key, 6), dim), (blocks,), jnp.float32, smallest / len(cuts), top_value / len(cuts))
        loudness = loudness * jnp.repeat(jnp.exp(draws), dims[dim] // blocks).reshape((-1,) + (1,) * (len(dims) - 1 - dim))
    return loudness


def split_up(amount, total, reach, slope):
    loads = [(1 << 20) // math.isqrt(grade ** slope) + 1 for grade in range(2, amount + 1)]
    spare, counts = total - reach - (amount - 1), [1] * (amount - 1)
    while spare > 0:
        free = [i for i in range(amount - 1) if counts[i] < reach]
        mass, left = sum([loads[i] for i in free]), spare
        for i in free:
            extra = min(reach - counts[i], max(1, left * loads[i] // mass), spare)
            counts[i] = counts[i] + extra
            spare = spare - extra
    return np.array([reach] + counts)


def ragged_sizes(stream_key, number_of, total, most, lean):
    if number_of == 2:
        one = jax.random.randint(stream_key, (), max(1, total - most), min(most, total - 1) + 1)
        return jnp.stack([one, total - one])
    sizes = jnp.asarray(split_up(number_of, total, most, lean), jnp.int32)
    couples = (number_of - 1) // 2
    giver, taker = sizes[1:1 + 2 * couples:2], sizes[2:2 + 2 * couples:2]
    slack = jnp.minimum(giver - 1, most - taker)
    moved = jax.random.randint(jax.random.fold_in(stream_key, 1), (couples,), 0, 1 << 20) % (slack + 1)
    sizes = sizes.at[1:1 + 2 * couples:2].set(giver - moved).at[2:2 + 2 * couples:2].set(taker + moved)
    return sizes[jax.random.permutation(jax.random.fold_in(stream_key, 2), number_of)]


def shared_out(own_key, own, number, rows, number_of, top, bound, skew):
    sequence = jax.random.permutation(own_key, number_of)
    packed, common = load_shares(number_of, rows * top, bound, skew, True), load_shares(number_of, rows * top, bound, skew, False)
    places = jnp.arange(number_of)

    def named(sizes, rotation):
        used = int((sizes > 0).sum())
        fixed = max(1, used // 4)
        shifted = fixed + (places - fixed + rotation * (used - fixed)) % max(1, number_of - fixed)
        return jnp.zeros((number_of,), jnp.int32).at[sequence[jnp.where(places < fixed, places, shifted)]].set(jnp.asarray(sizes, jnp.int32))

    sizes = jnp.where(number % 4 == 0, named(packed, number // 4), named(common, number - number // 4 - 1))
    mixed = jax.random.permutation(jax.random.fold_in(own, 3), number_of)
    source_of, taker = mixed[0:number_of // 2 * 2:2], mixed[1:number_of // 2 * 2:2]
    room = jnp.minimum(sizes[source_of] - 1, bound - sizes[taker]) // 2
    room = jnp.where((source_of == sequence[0]) | (taker == sequence[0]) | (sizes[taker] == 0), 0, jnp.maximum(room, 0))
    shifted = jax.random.randint(jax.random.fold_in(own, 4), (number_of // 2,), 0, 1 << 20) % (room + 1)
    sizes = sizes.at[source_of].add(-shifted).at[taker].add(shifted)
    labels = jnp.searchsorted(jnp.cumsum(sizes), jnp.arange(rows * top), side="right").astype(jnp.int32)
    table = labels.reshape(top, rows).T
    table = table[jax.random.permutation(jax.random.fold_in(own, 1), rows)]
    rotation = jax.random.randint(jax.random.fold_in(own, 2), (rows, 1), 0, top)
    return jnp.take_along_axis(table, (jnp.arange(top)[None, :] + rotation) % top, axis=1)


def load_shares(count, total, reach, lean, full):
    loads = [(1 << 20) // math.isqrt(rank ** lean) + 1 for rank in range(1, count + 1)]
    largest = reach if full else min(reach, max(-(-total // count), total * loads[0] // sum(loads)))
    least = 1 if total - largest >= count - 1 else 0
    holding, rest = [largest] + [least] * (count - 1), total - largest - least * (count - 1)
    while rest > 0:
        movable = [i for i in range(1, count) if holding[i] < largest] or [i for i in range(1, count) if holding[i] < reach]
        whole, left = sum([loads[i] for i in movable]), rest
        for i in movable:
            extra = min(reach - holding[i], max(1, left * loads[i] // whole), rest)
            holding[i] = holding[i] + extra
            rest = rest - extra
    return np.array(holding)


def normal_values(stream_key, extent, width, bound, cuts=(), kind=jnp.bfloat16):
    drawn = width * jax.random.normal(stream_key, extent, jnp.float32)
    if cuts:
        drawn = drawn * steps_of(stream_key, extent, cuts, -0.22, 0.18)
    return jnp.clip(drawn, -bound, bound).astype(kind)


def setup_inputs(seed: int = 0) -> dict:
    streams_of = jax.random.split(jax.random.key(seed), 20)
    tokens = normal_values(streams_of[0], (BATCH, D), 1.0, 6.0, ((0, 8),))
    kv_cache = draw_kv_cache(jax.random.fold_in(streams_of[19], 71), 0)
    lengths = ragged_sizes(streams_of[2], BATCH, BATCH * CACHE // 2, CACHE, 2).astype(jnp.int32)
    attn_gain = jnp.clip(1.0 + 0.18 * jax.random.normal(streams_of[3], (D,), jnp.float32), 0.1, 1.9)
    w_query = normal_values(streams_of[4], (D, HEADS * 2 * QK_DIM), D ** -0.5, 0.125, ((1, 4),))
    w_key = normal_values(streams_of[5], (D, KV_HEADS * 2 * QK_DIM), D ** -0.5, 0.125, ((1, 4),))
    w_value = normal_values(streams_of[6], (D, KV_HEADS * V_DIM), D ** -0.5, 0.125, ((1, 4),))
    lambdas = jnp.clip(0.3 + 0.5 * jax.random.uniform(streams_of[7], (HEADS,), jnp.float32) ** steps_of(streams_of[7], (HEADS,), ((0, 4),), -0.2, 0.2), 0.3, 0.8)
    head_gain = jnp.clip(1.0 + 0.18 * jax.random.normal(streams_of[8], (V_DIM,), jnp.float32), 0.1, 1.9)
    w_out = normal_values(streams_of[9], (HEADS * V_DIM, D), (HEADS * V_DIM) ** -0.5, 0.1875)
    ffn_gain = jnp.clip(1.0 + 0.18 * jax.random.normal(streams_of[10], (D,), jnp.float32), 0.1, 1.9)
    w_shared_gate = normal_values(streams_of[11], (D, FF_S), D ** -0.5, 0.125, ((1, 4),))
    w_shared_up = normal_values(streams_of[12], (D, FF_S), D ** -0.5, 0.125, ((1, 4),))
    w_shared_down = normal_values(streams_of[13], (FF_S, D), FF_S ** -0.5, 0.25, ((0, 4),))
    routing_keys = jax.random.split(jax.random.fold_in(streams_of[14], 1), BATCH // SEQ_DEV)
    routing_turns = jax.random.permutation(jax.random.fold_in(streams_of[14], 3), BATCH // SEQ_DEV)
    routing = jax.vmap(lambda own, number: shared_out(jax.random.fold_in(streams_of[14], 2), own, number, SEQ_DEV, EXPERTS, TOPK, CAP, 2))(routing_keys, routing_turns).reshape((BATCH, TOPK))
    route_weights = jnp.clip(jnp.exp(math.log(1.0) - 2.3025851 * jax.random.uniform(streams_of[15], (BATCH, TOPK), jnp.float32) ** steps_of(streams_of[15], (BATCH, TOPK), ((0, 8),), -0.2, 0.2)), 0.1, 1.0)
    w_exp_gate = normal_values(streams_of[16], (EXPERTS, D, FF_E), D ** -0.5, 0.125, ((0, 32),))
    w_exp_up = normal_values(streams_of[17], (EXPERTS, D, FF_E), D ** -0.5, 0.125, ((0, 32),))
    w_exp_down = normal_values(streams_of[18], (EXPERTS, FF_E, D), FF_E ** -0.5, 0.25, ((0, 32),))
    return {"tokens": tokens, "kv_cache": kv_cache, "lengths": lengths, "attn_gain": attn_gain, "w_query": w_query, "w_key": w_key, "w_value": w_value, "lambdas": lambdas, "head_gain": head_gain, "w_out": w_out, "ffn_gain": ffn_gain, "w_shared_gate": w_shared_gate, "w_shared_up": w_shared_up, "w_shared_down": w_shared_down, "routing": routing, "route_weights": route_weights, "w_exp_gate": w_exp_gate, "w_exp_up": w_exp_up, "w_exp_down": w_exp_down}


epsilon = 1e-06
neg_fill = -1e+30

def norm_rows(values, gain_vec):
    widened = values.astype(jnp.float32)
    return widened * lax.rsqrt(lax.optimization_barrier(jnp.mean(widened * widened, axis=-1, keepdims=True)) + epsilon) * gain_vec

def group_sum(inner_act, weight):
    row_count = inner_act.shape[0]
    pieces = jnp.einsum('mtf,tfd->mtd', inner_act.reshape(row_count, N_TP, -1).astype(jnp.float32), weight.reshape(N_TP, -1, weight.shape[-1]).astype(jnp.float32))
    rounded = lax.optimization_barrier(pieces.astype(jnp.bfloat16))
    return lax.optimization_barrier(jnp.sum(rounded.astype(jnp.float32), axis=1))

def attend(block_q, block_k, block_v, block_cache, block_len, lambdas, head_gain):
    seq_total = block_q.shape[0]
    v_width = head_gain.shape[0]
    qk_width = v_width // 2
    kv_total = block_cache.shape[2] // (2 * v_width)
    group_size = lambdas.shape[0] // kv_total
    cache_len = block_cache.shape[1]
    queries = block_q.reshape(seq_total, kv_total, group_size, 2, qk_width).astype(jnp.float32)
    key_new = block_k.reshape(seq_total, kv_total, 2, qk_width).astype(jnp.float32)
    value_new = block_v.reshape(seq_total, kv_total, v_width).astype(jnp.float32)
    layout = block_cache.reshape(seq_total, cache_len, kv_total, 2 * v_width)
    keys_old = layout[..., :v_width].reshape(seq_total, cache_len, kv_total, 2, qk_width).astype(jnp.float32)
    values_old = layout[..., v_width:].astype(jnp.float32)
    scaling = qk_width ** (-0.5)
    scores_old = jnp.einsum('skgmd,sckmd->skgmc', queries, keys_old) * scaling
    scores_new = jnp.einsum('skgmd,skmd->skgm', queries, key_new) * scaling
    position = jnp.arange(cache_len, dtype=jnp.int32)
    valid_mask = (position[None, :] < block_len[:, None])[:, None, None, None, :]
    scores_old = jnp.where(valid_mask, scores_old, neg_fill)
    highest = jnp.maximum(lax.optimization_barrier(jnp.max(scores_old, axis=-1)), scores_new)
    expo_old = jnp.where(valid_mask, jnp.exp(scores_old - highest[..., None]), 0.0)
    expo_new = jnp.exp(scores_new - highest)
    totals = lax.optimization_barrier(jnp.sum(expo_old, axis=-1)) + expo_new
    lambda_grid = lambdas.reshape(kv_total, group_size)[None, :, :]
    weight_old = (expo_old[..., 0, :] / totals[..., 0, None] - lambda_grid[..., None] * expo_old[..., 1, :] / totals[..., 1, None]).astype(jnp.bfloat16)
    weight_new = (expo_new[..., 0] / totals[..., 0] - lambda_grid * expo_new[..., 1] / totals[..., 1]).astype(jnp.bfloat16)
    head_mix = jnp.einsum('skgc,sckv->skgv', weight_old.astype(jnp.float32), values_old)
    head_mix = head_mix + weight_new.astype(jnp.float32)[..., None] * value_new[:, :, None, :]
    return norm_rows(head_mix, head_gain).astype(jnp.bfloat16).reshape(seq_total, -1)

def reference(tokens, kv_cache, lengths, attn_gain, w_query, w_key, w_value, lambdas, head_gain, w_out, ffn_gain, w_shared_gate, w_shared_up, w_shared_down, routing, route_weights, w_exp_gate, w_exp_up, w_exp_down):
    normed = norm_rows(tokens, attn_gain).astype(jnp.bfloat16)
    queries = jnp.dot(normed, w_query, preferred_element_type=jnp.float32).astype(jnp.bfloat16)
    key_new = jnp.dot(normed, w_key, preferred_element_type=jnp.float32).astype(jnp.bfloat16)
    value_new = jnp.dot(normed, w_value, preferred_element_type=jnp.float32).astype(jnp.bfloat16)

    def attend_block(operands):
        return attend(operands[0], operands[1], operands[2], operands[3], operands[4], lambdas, head_gain)
    head_out = lax.map(attend_block, (queries.reshape(N_EP, SEQ_DEV, -1), key_new.reshape(N_EP, SEQ_DEV, -1), value_new.reshape(N_EP, SEQ_DEV, -1), kv_cache.reshape(N_EP, SEQ_DEV, CACHE, -1), lengths.reshape(N_EP, SEQ_DEV)))
    head_out = head_out.reshape(BATCH, HEADS * V_DIM)
    projected = group_sum(head_out, w_out)
    residual = (tokens.astype(jnp.float32) + projected).astype(jnp.bfloat16)
    ffn_in = norm_rows(residual, ffn_gain).astype(jnp.bfloat16)
    gate_vals = jnp.dot(ffn_in, w_shared_gate, preferred_element_type=jnp.float32)
    up_vals = jnp.dot(ffn_in, w_shared_up, preferred_element_type=jnp.float32)
    shared_act = (jax.nn.silu(gate_vals) * up_vals).astype(jnp.bfloat16)
    shared = jnp.dot(shared_act, w_shared_down, preferred_element_type=jnp.float32)
    grouped_ids = routing.reshape(N_EP, SEQ_DEV * TOPK)
    onehot = (grouped_ids[..., None] == jnp.arange(EXPERTS, dtype=jnp.int32)).astype(jnp.int32)
    slot_rank = lax.optimization_barrier(jnp.sum((jnp.cumsum(onehot, axis=1) - onehot) * onehot, axis=-1)).astype(jnp.int32)
    group_ids = jnp.broadcast_to(jnp.arange(N_EP, dtype=jnp.int32)[:, None], slot_rank.shape)
    rows_in = jnp.repeat(ffn_in.reshape(N_EP, SEQ_DEV, D), TOPK, axis=1)
    buffers = jnp.zeros((EXPERTS, N_EP, CAP, D), jnp.bfloat16).at[grouped_ids, group_ids, slot_rank].set(rows_in)

    def expert_apply(operands):
        row_block, gate_w, up_w, down_w = operands
        flat_rows = row_block.reshape(N_EP * CAP, D)
        gate_part = jnp.dot(flat_rows, gate_w, preferred_element_type=jnp.float32)
        up_part = jnp.dot(flat_rows, up_w, preferred_element_type=jnp.float32)
        inner_act = (jax.nn.silu(gate_part) * up_part).astype(jnp.bfloat16)
        result = jnp.dot(inner_act, down_w, preferred_element_type=jnp.float32).astype(jnp.bfloat16)
        return result.reshape(N_EP, CAP, D)
    expert_res = lax.map(expert_apply, (buffers, w_exp_gate, w_exp_up, w_exp_down))
    picked = expert_res[grouped_ids, group_ids, slot_rank].astype(jnp.float32)
    routed = lax.optimization_barrier(jnp.sum(route_weights.reshape(N_EP, SEQ_DEV, TOPK, 1) * picked.reshape(N_EP, SEQ_DEV, TOPK, D), axis=2))
    routed = routed.reshape(BATCH, D)
    return (residual.astype(jnp.float32) + shared + routed).astype(jnp.bfloat16)
```

```python
import functools

import jax
import jax.numpy as jnp
from jax import lax
from jax.experimental import pallas as pl
from jax.experimental.pallas import tpu as pltpu
from jax.sharding import PartitionSpec as P

epsilon = 1e-06
neg_fill = -1e30
MESH = pl.DeviceIdType.MESH
F32 = jnp.float32
BF16 = jnp.bfloat16


def mm(left, right):
    return jnp.dot(left, right, preferred_element_type=F32)


def iota(shape, dim):
    return lax.broadcasted_iota(jnp.int32, shape, dim)


def hot(condition):
    return condition.astype(F32).astype(BF16)


def mm_t(left, right):
    return lax.dot_general(left, right, (((1,), (1,)), ((), ())), preferred_element_type=F32)


def exact(left, right, last):
    return lax.dot_general(
        left,
        right,
        (((1,), (last,)), ((), ())),
        preferred_element_type=F32,
        precision=lax.Precision.HIGHEST,
    )


def rms(values, gain):
    return values * lax.rsqrt(jnp.mean(values * values, axis=-1, keepdims=True) + epsilon) * gain


def flat_slots(values):
    blocks, rows, width = values.shape
    wide = values.astype(F32)
    if rows % 8 == 0:
        return wide.reshape(blocks * rows, width)
    return jnp.concatenate([wide[i] for i in range(blocks)], axis=0)


def layer(
    n_ep,
    n_tp,
    capacity,
    group,
    lengths_hbm,
    lambdas_hbm,
    tokens_hbm,
    attn_gain_hbm,
    head_gain_hbm,
    ffn_gain_hbm,
    routing_hbm,
    route_weights_hbm,
    kv_hbm,
    wq_hbm,
    wk_hbm,
    wv_hbm,
    wo_hbm,
    sg_hbm,
    su_hbm,
    sd_hbm,
    eg_hbm,
    eu_hbm,
    ed_hbm,
    out,
    lengths,
    lambdas,
    tokens,
    attn_gain,
    head_gain,
    ffn_gain,
    routing,
    route_weights,
    kv,
    wq,
    wk,
    wv,
    wo,
    sg,
    su,
    sd,
    eg,
    eu,
    ed,
    q_rows,
    score_new,
    value_new,
    mix_rows,
    heads,
    resid,
    packed,
    arrived,
    computed,
    returned,
    share_out,
    share_in,
    in_sem,
    kv_sem,
    w_sem,
    head_send,
    head_recv,
    disp_send,
    disp_recv,
    back_send,
    back_recv,
    share_send,
    share_recv,
):
    n_dev = n_ep * n_tp
    ep = lax.axis_index("ep")
    tp = lax.axis_index("tp")
    me = ep * n_tp + tp
    seqs, width = tokens.shape
    cache_len, lanes = kv.shape[1], kv.shape[2]
    v_width = lanes // 2
    qk_width = v_width // 2
    per_kv = lambdas.shape[0]
    side = lanes // v_width * 2
    packs = seqs // side
    half = side * per_kv
    block = 2 * half
    share = width // n_tp
    scaling = qk_width**-0.5
    barrier = pltpu.get_barrier_semaphore()

    inputs = [
        pltpu.make_async_copy(source, target, in_sem.at[i])
        for i, (source, target) in enumerate(
            [
                (tokens_hbm, tokens),
                (attn_gain_hbm, attn_gain),
                (routing_hbm, routing),
                (route_weights_hbm, route_weights),
                (head_gain_hbm, head_gain),
                (lambdas_hbm, lambdas),
                (lengths_hbm, lengths),
                (ffn_gain_hbm, ffn_gain),
            ]
        )
    ]
    weights = [
        pltpu.make_async_copy(src, dst, w_sem.at[i])
        for i, (src, dst) in enumerate(
            [
                (wq_hbm, wq),
                (wk_hbm, wk),
                (wv_hbm, wv),
                (wo_hbm, wo),
                (sg_hbm, sg),
                (su_hbm, su),
                (sd_hbm, sd),
                (eg_hbm.at[0], eg),
                (eu_hbm.at[0], eu),
                (ed_hbm.at[0], ed),
            ]
        )
    ]

    def kv_copy(pack):
        rows = pl.ds(side * pack, side)
        return pltpu.make_async_copy(kv_hbm.at[rows], kv.at[rows], kv_sem.at[pack])

    inputs[0].start()
    inputs[1].start()
    for i in range(3):
        weights[i].start()
    for i in range(2, 8):
        inputs[i].start()

    def greet(step, carry):
        other = lax.rem(me + step, n_dev)
        pl.semaphore_signal(
            barrier, inc=1, device_id=(other // n_tp, lax.rem(other, n_tp)), device_id_type=MESH
        )
        return carry

    lax.fori_loop(1, n_dev, greet, 0)

    def start_kv(pack, carry):
        kv_copy(pack).start()
        return carry

    lax.fori_loop(0, packs, start_kv, 0)

    for i in range(2):
        inputs[i].wait()
    normed = rms(tokens[...].astype(F32), attn_gain[...]).astype(BF16)
    top_count, batch = routing.shape
    picked = (iota((seqs, batch), 0) + ep * seqs == iota((seqs, batch), 1)).astype(F32)
    for i in range(2, 4):
        inputs[i].wait()
    own_ids = exact(picked, routing[...].astype(F32), 1).astype(jnp.int32)
    own_weights = exact(
        (iota((seqs, seqs), 0) == iota((seqs, seqs), 1)).astype(F32), route_weights[...], 1
    )
    before = hot(iota((seqs, seqs), 1) < iota((seqs, seqs), 0))

    def slots(count, expert_of):
        column = iota((seqs, count), 1)
        expert = expert_of(column // capacity)
        named = [own_ids[:, k : k + 1] == expert for k in range(top_count)]
        hit = functools.reduce(jnp.logical_or, named)
        rank = mm(before, hot(hit))
        chosen = hit & (rank == lax.rem(column, capacity).astype(F32))
        return named, chosen

    _, chosen = slots(n_ep * capacity, lambda target: target * n_tp + tp)
    dispatch = hot(chosen)
    named_all, chosen_all = slots(n_dev * capacity, lambda expert: expert)
    mixing = jnp.zeros((seqs, n_dev * capacity), F32)
    for k in range(top_count):
        mixing = mixing + jnp.where(named_all[k] & chosen_all, own_weights[:, k : k + 1], 0.0)
    mix_high = mixing.astype(BF16)
    mix_low = (mixing - mix_high.astype(F32)).astype(BF16)

    for i in range(3):
        weights[i].wait()
    queries = mm(normed, wq[...]).astype(BF16)
    key_new = mm_t(normed, wk[...]).astype(BF16)
    val_new = mm_t(normed, wv[...]).astype(BF16)
    fold_width = side * v_width
    spot = (v_width, fold_width)
    tile = hot(iota(spot, 0) == lax.rem(iota(spot, 1), v_width))

    rows = seqs * 2 * per_kv
    row = iota((rows, seqs), 0)
    spread = hot(row // block * side + lax.rem(row, half) // per_kv == iota((rows, seqs), 1))
    wide_q = mm(spread, queries)
    row = iota(wide_q.shape, 0)
    lane = iota(wide_q.shape, 1)
    mine = (lane // v_width == lax.rem(row, per_kv)) & (
        lax.rem(lane, v_width) // qk_width == lax.rem(row, block) // half
    )
    wide_q = jnp.where(mine, wide_q, 0.0).astype(BF16)
    fold = (queries.shape[1], fold_width)
    folded = mm(wide_q, hot(lax.rem(iota(fold, 0), v_width) == lax.rem(iota(fold, 1), v_width)))
    row = iota(folded.shape, 0)
    lane = iota(folded.shape, 1)
    folded = jnp.where(lax.rem(row, half) // per_kv == lane // v_width, folded, 0.0)
    q_rows[...] = folded.astype(BF16)
    keys_wide = mm(spread, mm(key_new, tile).astype(BF16))
    fresh = jnp.sum(folded * keys_wide, axis=1, keepdims=True)
    score_new[...] = jnp.broadcast_to(fresh, score_new.shape)
    row = iota((seqs * per_kv, seqs), 0)
    repeat = hot(row // per_kv == iota((seqs * per_kv, seqs), 1))
    value_new[...] = mm(repeat, mm(val_new, tile).astype(BF16))

    for i in range(4, 8):
        inputs[i].wait()
    wide_gain = exact(jnp.broadcast_to(head_gain[...], (8, v_width)), tile.astype(F32), 0)
    row = iota((block, 1), 0)
    factor = jnp.ones((block, 1), F32)
    for g in range(per_kv):
        factor = jnp.where((row >= half) & (lax.rem(row, per_kv) == g), lambdas[g], factor)

    for i in range(3, 10):
        weights[i].start()

    def attend(index, carry):
        first = index * group
        for i in range(group):
            kv_copy(first + i).wait()
        stage = []
        values = []
        for i in range(group):
            pack = first + i
            keys = []
            swapped = []
            for j in range(0, side, 2):
                even = kv[side * pack + j]
                odd = pltpu.roll(kv[side * pack + j + 1], v_width, 1)
                keys += [even[:, :v_width], odd[:, v_width:]]
                swapped += [odd[:, :v_width], even[:, v_width:]]
            keys = jnp.concatenate(keys, axis=1)
            values.append(jnp.concatenate(swapped, axis=1))
            query = q_rows[pl.ds(pl.multiple_of(pack * block, block), block), :]
            stage.append(mm_t(query, keys))
        weighed = []
        for i in range(group):
            pack = first + i
            fresh = score_new[pl.ds(pl.multiple_of(pack * block, block), block), :][:, :1]
            owner = lax.rem(iota((block, 1), 0), half) // per_kv
            limit = jnp.zeros((block, 1), jnp.int32)
            for j in range(side):
                limit = jnp.where(owner == j, lengths[side * pack + j], limit)
            valid = iota((block, cache_len), 1) < limit
            scores = jnp.where(valid, stage[i], neg_fill)
            highest = jnp.maximum(jnp.max(scores, axis=1, keepdims=True), fresh)
            expo = jnp.exp((scores - highest) * scaling)
            expo_new = jnp.exp((fresh - highest) * scaling)
            scale = factor / (jnp.sum(expo, axis=1, keepdims=True) + expo_new)
            expo = expo * scale
            expo_new = expo_new * scale
            weighed.append(
                (
                    (expo[:half] - expo[half:]).astype(BF16),
                    (expo_new[:half] - expo_new[half:]).astype(BF16).astype(F32),
                )
            )
        for i in range(group):
            pack = first + i
            spots = pl.ds(pl.multiple_of(pack * half, half), half)
            mixed = mm(weighed[i][0], values[i]) + weighed[i][1] * value_new[spots, :]
            owner = iota(mixed.shape, 0) // per_kv
            own = owner + 1 - 2 * lax.rem(owner, 2) == iota(mixed.shape, 1) // v_width
            mix_rows[spots, :] = jnp.where(own, mixed, 0.0)
        return carry

    lax.fori_loop(0, packs // group, attend, 0)

    mixed = mix_rows[...]
    mean = jnp.sum(mixed * mixed, axis=1, keepdims=True) * (1.0 / v_width)
    head_out = (mixed * lax.rsqrt(mean + epsilon) * wide_gain[:1]).astype(BF16)
    unfold = (fold_width, per_kv * v_width)
    shifted = hot(lax.rem(iota(unfold, 1), v_width) == lax.rem(iota(unfold, 0), v_width))
    laid = mm(head_out, shifted)
    own = iota(laid.shape, 1) // v_width == lax.rem(iota(laid.shape, 0), per_kv)
    laid = jnp.where(own, laid, 0.0).astype(BF16)
    gather = (seqs, seqs * per_kv)
    heads[tp] = mm(hot(iota(gather, 1) // per_kv == iota(gather, 0)), laid).astype(BF16)

    pl.semaphore_wait(barrier, n_dev - 1)

    def head_copy(step):
        other = lax.rem(tp + step, n_tp)
        return pltpu.make_async_remote_copy(
            src_ref=heads.at[tp],
            dst_ref=heads.at[tp],
            send_sem=head_send.at[step],
            recv_sem=head_recv.at[step],
            device_id=(ep, other),
            device_id_type=MESH,
        )

    head_copies = [head_copy(step) for step in range(1, n_tp)]
    for copy in head_copies:
        copy.start()
    weights[3].wait()
    for copy in head_copies:
        copy.wait_recv()
    depth = heads.shape[2]
    projected = jnp.zeros((seqs, width), F32)
    for i in range(n_tp):
        piece = mm(heads[i], wo[i * depth : (i + 1) * depth, :])
        projected = projected + piece.astype(BF16).astype(F32)
    residual = (tokens[...].astype(F32) + projected).astype(BF16).astype(F32)
    for i in range(n_tp):
        resid[i] = residual[:, i * share : (i + 1) * share]
    ffn_in = rms(residual, ffn_gain[...]).astype(BF16)

    sorted_rows = lax.dot_general(
        dispatch, ffn_in, (((0,), (0,)), ((), ())), preferred_element_type=F32
    )
    for e in range(n_ep):
        packed[e] = sorted_rows[e * capacity : (e + 1) * capacity, :].astype(BF16)
    arrived[ep] = packed[ep]

    def disp_copy(step):
        other = lax.rem(ep + step, n_ep)
        return pltpu.make_async_remote_copy(
            src_ref=packed.at[other],
            dst_ref=arrived.at[ep],
            send_sem=disp_send.at[step],
            recv_sem=disp_recv.at[step],
            device_id=(other, tp),
            device_id_type=MESH,
        )

    def loop(make, act, count):
        def body(step, carry):
            act(make(step))
            return carry

        lax.fori_loop(1, count, body, 0)

    loop(disp_copy, lambda copy: copy.start(), n_ep)

    for i in range(4, 7):
        weights[i].wait()
    shared_act = (jax.nn.silu(mm(ffn_in, sg[...])) * mm(ffn_in, su[...])).astype(BF16)
    shared_part = mm(shared_act, sd[...])
    for i in range(n_tp):
        share_out[i] = shared_part[:, i * share : (i + 1) * share].astype(BF16)

    def share_copy(step):
        other = lax.rem(tp + step, n_tp)
        return pltpu.make_async_remote_copy(
            src_ref=share_out.at[other],
            dst_ref=share_in.at[step],
            send_sem=share_send.at[step],
            recv_sem=share_recv.at[step],
            device_id=(ep, other),
            device_id_type=MESH,
        )

    share_copies = [share_copy(step) for step in range(1, n_tp)]
    for copy in share_copies:
        copy.start()

    for i in range(7, 10):
        weights[i].wait()
    loop(disp_copy, lambda copy: copy.wait_recv(), n_ep)
    flat = flat_slots(arrived[...]).astype(BF16)
    act = (jax.nn.silu(mm(flat, eg[...])) * mm(flat, eu[...])).astype(BF16)
    result = mm(act, ed[...])
    for e in range(n_ep):
        for t in range(n_tp):
            computed[e * n_tp + t] = result[
                e * capacity : (e + 1) * capacity, t * share : (t + 1) * share
            ].astype(BF16)
    returned[me] = computed[me]

    def back_copy(step):
        other = lax.rem(me + step, n_dev)
        return pltpu.make_async_remote_copy(
            src_ref=computed.at[other],
            dst_ref=returned.at[me],
            send_sem=back_send.at[step],
            recv_sem=back_recv.at[step],
            device_id=(other // n_tp, lax.rem(other, n_tp)),
            device_id_type=MESH,
        )

    loop(back_copy, lambda copy: copy.start(), n_dev)
    total = resid[tp] + share_out[tp].astype(F32)
    for step, copy in enumerate(share_copies):
        copy.wait_recv()
        total = total + share_in[step + 1].astype(F32)
    loop(back_copy, lambda copy: copy.wait_recv(), n_dev)
    back = flat_slots(returned[...]).astype(BF16)
    routed = mm(mix_high, back) + mm(mix_low, back)
    out[...] = (total + routed).astype(BF16)

    for copy in head_copies + share_copies:
        copy.wait_send()
    loop(disp_copy, lambda copy: copy.wait_send(), n_ep)
    loop(back_copy, lambda copy: copy.wait_send(), n_dev)


def shards(
    n_ep,
    n_tp,
    tokens,
    kv_cache,
    lengths,
    attn_gain,
    w_query,
    w_key,
    w_value,
    lambdas,
    head_gain,
    w_out,
    ffn_gain,
    w_shared_gate,
    w_shared_up,
    w_shared_down,
    routing,
    route_weights,
    w_exp_gate,
    w_exp_up,
    w_exp_down,
):
    seqs, width = tokens.shape
    lanes = kv_cache.shape[2]
    v_width = head_gain.shape[0]
    per_kv = lambdas.shape[0]
    n_dev = n_ep * n_tp
    capacity = max(2, 2 * seqs * routing.shape[1] // (w_exp_gate.shape[0] * n_dev))
    share = width // n_tp
    side = lanes // v_width * 2
    packs = seqs // side
    rows = seqs * per_kv
    fold = side * v_width
    group = next(g for g in (4, 2, 1) if packs % g == 0)
    small = [
        lengths,
        lambdas,
        tokens,
        attn_gain[None, :],
        head_gain[None, :],
        ffn_gain[None, :],
        routing.T,
        route_weights.T,
    ]
    big = [
        kv_cache,
        w_query,
        w_key.T,
        w_value.T,
        w_out,
        w_shared_gate,
        w_shared_up,
        w_shared_down,
        w_exp_gate,
        w_exp_up,
        w_exp_down,
    ]
    held = [pltpu.SMEM(x.shape, x.dtype) for x in small[:2]]
    held += [pltpu.VMEM(x.shape, x.dtype) for x in small[2:]]
    held += [pltpu.VMEM(x.shape, BF16) for x in big[:8]]
    held += [pltpu.VMEM(x.shape[1:], BF16) for x in big[8:]]
    vmem = pl.BlockSpec(memory_space=pltpu.VMEM)
    dma = pltpu.SemaphoreType.DMA
    return pl.pallas_call(
        functools.partial(layer, n_ep, n_tp, capacity, group),
        out_shape=pltpu.VMEM((seqs, share), BF16),
        in_specs=[pl.BlockSpec(memory_space=pltpu.HBM)] * (len(small) + len(big)),
        out_specs=vmem,
        scratch_shapes=held
        + [
            pltpu.VMEM((2 * rows, fold), BF16),
            pltpu.VMEM((2 * rows, lanes), F32),
            pltpu.VMEM((rows, fold), F32),
            pltpu.VMEM((rows, fold), F32),
            pltpu.VMEM((n_tp, seqs, per_kv * v_width), BF16),
            pltpu.VMEM((n_tp, seqs, share), F32),
            pltpu.VMEM((n_ep, capacity, width), BF16),
            pltpu.VMEM((n_ep, capacity, width), BF16),
            pltpu.VMEM((n_dev, capacity, share), BF16),
            pltpu.VMEM((n_dev, capacity, share), BF16),
            pltpu.VMEM((n_tp, seqs, share), BF16),
            pltpu.VMEM((n_tp, seqs, share), BF16),
            dma((len(small),)),
            dma((packs,)),
            dma((10,)),
            dma((n_tp,)),
            dma((n_tp,)),
            dma((n_ep,)),
            dma((n_ep,)),
            dma((n_dev,)),
            dma((n_dev,)),
            dma((n_tp,)),
            dma((n_tp,)),
        ],
        compiler_params=pltpu.CompilerParams(
            collective_id=0, has_side_effects=True, vmem_limit_bytes=60 * 1024 * 1024
        ),
    )(
        *small,
        *big,
    )


def solution(mesh):
    return jax.shard_map(
        functools.partial(shards, mesh.shape["ep"], mesh.shape["tp"]),
        mesh=mesh,
        in_specs=(
            P("ep", None),
            P("ep", None, "tp"),
            P("ep"),
            P(),
            P(None, "tp"),
            P(None, "tp"),
            P(None, "tp"),
            P("tp"),
            P(),
            P(),
            P(),
            P(None, "tp"),
            P(None, "tp"),
            P("tp", None),
            P(),
            P("ep", None),
            P(("ep", "tp"), None, None),
            P(("ep", "tp"), None, None),
            P(("ep", "tp"), None, None),
        ),
        out_specs=P("ep", "tp"),
        check_vma=False,
    )
```

```python
import functools

import jax
import jax.numpy as jnp
from jax import lax
from jax.experimental import pallas as pl
from jax.experimental.pallas import tpu as pltpu
from jax.sharding import PartitionSpec as P

epsilon = 1e-06
neg_fill = -1e30
MESH = pl.DeviceIdType.MESH
F32 = jnp.float32
BF16 = jnp.bfloat16


def mm(left, right):
    return jnp.dot(left, right, preferred_element_type=F32)


def iota(shape, dim):
    return lax.broadcasted_iota(jnp.int32, shape, dim)


def hot(condition):
    return condition.astype(F32).astype(BF16)


def mm_t(left, right):
    return lax.dot_general(left, right, (((1,), (1,)), ((), ())), preferred_element_type=F32)


def exact(left, right, last):
    return lax.dot_general(
        left,
        right,
        (((1,), (last,)), ((), ())),
        preferred_element_type=F32,
        precision=lax.Precision.HIGHEST,
    )


def rms(values, gain):
    return values * lax.rsqrt(jnp.mean(values * values, axis=-1, keepdims=True) + epsilon) * gain


def flat_slots(values):
    blocks, rows, width = values.shape
    wide = values.astype(F32)
    if rows % 8 == 0:
        return wide.reshape(blocks * rows, width)
    return jnp.concatenate([wide[i] for i in range(blocks)], axis=0)


def layer(
    n_ep,
    n_tp,
    capacity,
    group,
    lengths_hbm,
    lambdas_hbm,
    tokens_hbm,
    attn_gain_hbm,
    head_gain_hbm,
    ffn_gain_hbm,
    routing_hbm,
    route_weights_hbm,
    kv_hbm,
    wq_hbm,
    wk_hbm,
    wv_hbm,
    wo_hbm,
    sg_hbm,
    su_hbm,
    sd_hbm,
    eg_hbm,
    eu_hbm,
    ed_hbm,
    out,
    lengths,
    lambdas,
    tokens,
    attn_gain,
    head_gain,
    ffn_gain,
    routing,
    route_weights,
    kv,
    wq,
    wk,
    wv,
    wo,
    sg,
    su,
    sd,
    eg,
    eu,
    ed,
    q_rows,
    score_new,
    value_new,
    mix_rows,
    heads,
    head_rows,
    head_slots,
    resid,
    relay_pick,
    relay,
    packed,
    arrived,
    computed,
    returned,
    share_out,
    share_in,
    in_sem,
    kv_sem,
    w_sem,
    head_sem,
    slot_sem,
    relay_sem,
    disp_sem,
    back_sem,
    share_sem,
):
    n_dev = n_ep * n_tp
    ep = lax.axis_index("ep")
    tp = lax.axis_index("tp")
    me = ep * n_tp + tp
    n_hi, plane = packed.shape[:2]
    n_lo = n_ep // n_hi
    hi = ep // n_lo
    lo = lax.rem(ep, n_lo)
    spot_in_plane = lo * n_tp + tp
    seqs, width = tokens.shape
    cache_len, lanes = kv.shape[1], kv.shape[2]
    v_width = lanes // 2
    qk_width = v_width // 2
    per_kv = lambdas.shape[0]
    side = lanes // v_width * 2
    packs = seqs // side
    half = side * per_kv
    block = 2 * half
    share = width // n_tp
    scaling = qk_width**-0.5
    barrier = pltpu.get_barrier_semaphore()

    inputs = [
        pltpu.make_async_copy(source, target, in_sem.at[i])
        for i, (source, target) in enumerate(
            [
                (tokens_hbm, tokens),
                (attn_gain_hbm, attn_gain),
                (routing_hbm, routing),
                (route_weights_hbm, route_weights),
                (head_gain_hbm, head_gain),
                (lambdas_hbm, lambdas),
                (lengths_hbm, lengths),
                (ffn_gain_hbm, ffn_gain),
            ]
        )
    ]
    weights = [
        pltpu.make_async_copy(src, dst, w_sem.at[i])
        for i, (src, dst) in enumerate(
            [
                (wq_hbm, wq),
                (wk_hbm, wk),
                (wv_hbm, wv),
                (wo_hbm, wo),
                (sg_hbm, sg),
                (su_hbm, su),
                (sd_hbm, sd),
                (eg_hbm.at[0], eg),
                (eu_hbm.at[0], eu),
                (ed_hbm.at[0], ed),
            ]
        )
    ]

    def kv_copy(pack):
        rows = pl.ds(side * pack, side)
        return pltpu.make_async_copy(kv_hbm.at[rows], kv.at[rows], kv_sem.at[pack])

    inputs[0].start()
    inputs[1].start()
    for i in range(3):
        weights[i].start()
    for i in range(2, 8):
        inputs[i].start()

    def greet(step, carry):
        other = lax.rem(me + step, n_dev)
        pl.semaphore_signal(
            barrier, inc=1, device_id=(other // n_tp, lax.rem(other, n_tp)), device_id_type=MESH
        )
        return carry

    lax.fori_loop(1, n_dev, greet, 0)

    def start_kv(pack, carry):
        kv_copy(pack).start()
        return carry

    lax.fori_loop(0, packs, start_kv, 0)

    def remote(source, target, sem, other_ep, other_tp):
        return pltpu.make_async_remote_copy(
            src_ref=source,
            dst_ref=target,
            send_sem=sem.at[0],
            recv_sem=sem.at[1],
            device_id=(other_ep, other_tp),
            device_id_type=MESH,
        )

    def whole(source, target, sem, count):
        part = pl.ds(0, count)
        return remote(
            source.at[part], target.at[part], sem, lax.rem(ep + 1, n_ep), lax.rem(tp + 1, n_tp)
        )

    def far_first(step, mine, count):
        late = 2 * mine // count
        up = count - 1 - step
        up = up - (mine >= up).astype(jnp.int32)
        down = step + (step >= mine).astype(jnp.int32)
        return (1 - late) * up + late * down

    peers = [
        (far_first(k, ep, n_ep), lax.rem(tp + t, n_tp))
        for k in range(n_ep - 1)
        for t in range(n_tp)
    ]
    peers += [(ep, lax.rem(tp + t, n_tp)) for t in range(1, n_tp)]
    far_planes = [far_first(k, hi, n_hi) for k in range(n_hi - 1)]

    def relay_copy(source, target):
        return pltpu.make_async_remote_copy(
            src_ref=tokens.at[:, pl.ds(pl.multiple_of(tp * share, share), share)],
            dst_ref=relay.at[source],
            send_sem=relay_sem.at[0],
            recv_sem=relay_sem.at[1 + source],
            device_id=(target * n_lo + lo, tp),
            device_id_type=MESH,
        )

    for i in range(2):
        inputs[i].wait()
    normed = rms(tokens[...].astype(F32), attn_gain[...]).astype(BF16)
    top_count, batch = routing.shape
    picked = (iota((seqs, batch), 0) + ep * seqs == iota((seqs, batch), 1)).astype(F32)
    for i in range(2, 4):
        inputs[i].wait()
    own_ids = exact(picked, routing[...].astype(F32), 1).astype(jnp.int32)
    own_weights = exact(
        (iota((seqs, seqs), 0) == iota((seqs, seqs), 1)).astype(F32), route_weights[...], 1
    )
    before = hot(iota((seqs, seqs), 1) < iota((seqs, seqs), 0))

    def slots(count, expert_of):
        column = iota((seqs, count), 1)
        expert = expert_of(column // capacity)
        named = [own_ids[:, k : k + 1] == expert for k in range(top_count)]
        hit = functools.reduce(jnp.logical_or, named)
        rank = mm(before, hot(hit))
        chosen = hit & (rank == lax.rem(column, capacity).astype(F32))
        return named, chosen

    named_all, chosen_all = slots(n_dev * capacity, lambda expert: expert)
    mixing = jnp.zeros((seqs, n_dev * capacity), F32)
    for k in range(top_count):
        mixing = mixing + jnp.where(named_all[k] & chosen_all, own_weights[:, k : k + 1], 0.0)
    row = iota((seqs * per_kv, seqs), 0)
    repeat = hot(row // per_kv == iota((seqs * per_kv, seqs), 1))
    row_choice = mm(repeat, hot(chosen_all)).astype(BF16)
    relayed = n_hi * seqs
    row = iota((relayed, batch), 0)
    picked = (row // seqs * n_lo + lo) * seqs + lax.rem(row, seqs) == iota((relayed, batch), 1)
    relay_ids = exact(picked.astype(F32), routing[...].astype(F32), 1).astype(jnp.int32)
    column = iota((relayed, plane * capacity), 1)
    expert = hi * plane + column // capacity
    hit = functools.reduce(
        jnp.logical_or, [relay_ids[:, k : k + 1] == expert for k in range(top_count)]
    )
    row, other = iota((relayed, relayed), 0), iota((relayed, relayed), 1)
    earlier = hot((row // seqs == other // seqs) & (other < row))
    chosen = hit & (mm(earlier, hot(hit)) == lax.rem(column, capacity).astype(F32))
    chosen = hot(chosen)
    for i in range(n_hi):
        relay_pick[i] = chosen[i * seqs : (i + 1) * seqs, :]
    mix_high = mixing.astype(BF16)
    mix_low = (mixing - mix_high.astype(F32)).astype(BF16)

    for i in range(3):
        weights[i].wait()
    queries = mm(normed, wq[...]).astype(BF16)
    key_new = mm_t(normed, wk[...]).astype(BF16)
    val_new = mm_t(normed, wv[...]).astype(BF16)
    fold_width = side * v_width
    spot = (v_width, fold_width)
    tile = hot(iota(spot, 0) == lax.rem(iota(spot, 1), v_width))

    rows = seqs * 2 * per_kv
    row = iota((rows, seqs), 0)
    spread = hot(row // block * side + lax.rem(row, half) // per_kv == iota((rows, seqs), 1))
    wide_q = mm(spread, queries)
    row = iota(wide_q.shape, 0)
    lane = iota(wide_q.shape, 1)
    mine = (lane // v_width == lax.rem(row, per_kv)) & (
        lax.rem(lane, v_width) // qk_width == lax.rem(row, block) // half
    )
    wide_q = jnp.where(mine, wide_q, 0.0).astype(BF16)
    fold = (queries.shape[1], fold_width)
    folded = mm(wide_q, hot(lax.rem(iota(fold, 0), v_width) == lax.rem(iota(fold, 1), v_width)))
    row = iota(folded.shape, 0)
    lane = iota(folded.shape, 1)
    folded = jnp.where(lax.rem(row, half) // per_kv == lane // v_width, folded, 0.0)
    q_rows[...] = folded.astype(BF16)
    keys_wide = mm(spread, mm(key_new, tile).astype(BF16))
    fresh = jnp.sum(folded * keys_wide, axis=1, keepdims=True)
    score_new[...] = jnp.broadcast_to(fresh, score_new.shape)
    value_new[...] = mm(repeat, mm(val_new, tile).astype(BF16))

    for i in range(4, 8):
        inputs[i].wait()
    wide_gain = exact(jnp.broadcast_to(head_gain[...], (8, v_width)), tile.astype(F32), 0)
    row = iota((block, 1), 0)
    factor = jnp.ones((block, 1), F32)
    for g in range(per_kv):
        factor = jnp.where((row >= half) & (lax.rem(row, per_kv) == g), lambdas[g], factor)

    for i in range(3, 10):
        weights[i].start()

    def attend(index, carry):
        first = index * group
        for i in range(group):
            kv_copy(first + i).wait()
        stage = []
        values = []
        for i in range(group):
            pack = first + i
            keys = []
            swapped = []
            for j in range(0, side, 2):
                even = kv[side * pack + j]
                odd = pltpu.roll(kv[side * pack + j + 1], v_width, 1)
                keys += [even[:, :v_width], odd[:, v_width:]]
                swapped += [odd[:, :v_width], even[:, v_width:]]
            keys = jnp.concatenate(keys, axis=1)
            values.append(jnp.concatenate(swapped, axis=1))
            query = q_rows[pl.ds(pl.multiple_of(pack * block, block), block), :]
            stage.append(mm_t(query, keys))
        weighed = []
        for i in range(group):
            pack = first + i
            fresh = score_new[pl.ds(pl.multiple_of(pack * block, block), block), :][:, :1]
            owner = lax.rem(iota((block, 1), 0), half) // per_kv
            limit = jnp.zeros((block, 1), jnp.int32)
            for j in range(side):
                limit = jnp.where(owner == j, lengths[side * pack + j], limit)
            valid = iota((block, cache_len), 1) < limit
            scores = jnp.where(valid, stage[i], neg_fill)
            highest = jnp.maximum(jnp.max(scores, axis=1, keepdims=True), fresh)
            expo = jnp.exp((scores - highest) * scaling)
            expo_new = jnp.exp((fresh - highest) * scaling)
            scale = factor / (jnp.sum(expo, axis=1, keepdims=True) + expo_new)
            expo = expo * scale
            expo_new = expo_new * scale
            weighed.append(
                (
                    (expo[:half] - expo[half:]).astype(BF16),
                    (expo_new[:half] - expo_new[half:]).astype(BF16).astype(F32),
                )
            )
        for i in range(group):
            pack = first + i
            spots = pl.ds(pl.multiple_of(pack * half, half), half)
            mixed = mm(weighed[i][0], values[i]) + weighed[i][1] * value_new[spots, :]
            owner = iota(mixed.shape, 0) // per_kv
            own = owner + 1 - 2 * lax.rem(owner, 2) == iota(mixed.shape, 1) // v_width
            mix_rows[spots, :] = jnp.where(own, mixed, 0.0)
        return carry

    def open_links():
        pl.semaphore_wait(barrier, n_dev - 1)
        for other in far_planes:
            relay_copy(hi, other).start()

    first_part = packs // group // 2
    lax.fori_loop(0, first_part, attend, 0)
    pl.when(me >= 2)(open_links)
    lax.fori_loop(first_part, packs // group, attend, 0)
    pl.when(me < 2)(open_links)

    mixed = mix_rows[...]
    mean = jnp.sum(mixed * mixed, axis=1, keepdims=True) * (1.0 / v_width)
    head_out = (mixed * lax.rsqrt(mean + epsilon) * wide_gain[:1]).astype(BF16)
    unfold = (fold_width, per_kv * v_width)
    shifted = hot(lax.rem(iota(unfold, 1), v_width) == lax.rem(iota(unfold, 0), v_width))
    laid = mm(head_out, shifted)
    own = iota(laid.shape, 1) // v_width == lax.rem(iota(laid.shape, 0), per_kv)
    laid = jnp.where(own, laid, 0.0).astype(BF16)
    picked_rows = lax.dot_general(
        row_choice, laid, (((0,), (0,)), ((), ())), preferred_element_type=F32
    )
    for e in range(n_dev):
        head_rows[e] = picked_rows[e * capacity : (e + 1) * capacity, :].astype(BF16)
    head_slots[tp * n_ep + ep] = head_rows[me]
    for other_ep, other_tp in peers:
        remote(
            head_rows.at[other_ep * n_tp + other_tp],
            head_slots.at[tp * n_ep + ep],
            slot_sem,
            other_ep,
            other_tp,
        ).start()
    gather = (seqs, seqs * per_kv)
    heads[tp] = mm(hot(iota(gather, 1) // per_kv == iota(gather, 0)), laid).astype(BF16)

    for t in range(1, n_tp):
        remote(heads.at[tp], heads.at[tp], head_sem, ep, lax.rem(tp + t, n_tp)).start()
    relay[hi] = tokens[:, pl.ds(pl.multiple_of(tp * share, share), share)]
    for index, source in enumerate([hi] + far_planes[::-1]):
        if index:
            relay_copy(source, lax.rem(hi + 1, n_hi)).wait_recv()
        rows_out = lax.dot_general(
            relay_pick[source], relay[source], (((0,), (0,)), ((), ())), preferred_element_type=F32
        )
        for q in range(plane):
            packed[source, q] = rows_out[q * capacity : (q + 1) * capacity, :].astype(BF16)
        arrived[tp, source, lo] = packed[source, spot_in_plane]
        for q in range(1, plane):
            other = lax.rem(spot_in_plane + q, plane)
            remote(
                packed.at[source, other],
                arrived.at[tp, source, lo],
                disp_sem,
                hi * n_lo + other // n_tp,
                lax.rem(other, n_tp),
            ).start()
    weights[3].wait()
    whole(heads, heads, head_sem, n_tp - 1).wait_recv()
    depth = heads.shape[2]
    projected = jnp.zeros((seqs, width), F32)
    for i in range(n_tp):
        piece = mm(heads[i], wo[i * depth : (i + 1) * depth, :])
        projected = projected + piece.astype(BF16).astype(F32)
    residual = (tokens[...].astype(F32) + projected).astype(BF16).astype(F32)
    for i in range(n_tp):
        resid[i] = residual[:, i * share : (i + 1) * share]
    ffn_in = rms(residual, ffn_gain[...]).astype(BF16)

    for i in range(4, 7):
        weights[i].wait()
    shared_act = (jax.nn.silu(mm(ffn_in, sg[...])) * mm(ffn_in, su[...])).astype(BF16)
    shared_part = mm(shared_act, sd[...])
    for i in range(n_tp):
        share_out[i] = shared_part[:, i * share : (i + 1) * share].astype(BF16)

    for t in range(1, n_tp):
        other = lax.rem(tp + t, n_tp)
        remote(share_out.at[other], share_in.at[t - 1], share_sem, ep, other).start()

    whole(head_rows, head_slots, slot_sem, n_dev - 1).wait_recv()
    projected = jnp.zeros((n_ep * capacity, width), F32)
    for i in range(n_tp):
        piece = flat_slots(head_slots[i * n_ep : (i + 1) * n_ep]).astype(BF16)
        piece = mm(piece, wo[i * depth : (i + 1) * depth, :])
        projected = projected + piece.astype(BF16).astype(F32)
    relayed_all = packed.at[:, pl.ds(0, plane - 1)]
    remote(relayed_all, relayed_all, disp_sem, ep, lax.rem(tp + 1, n_tp)).wait_recv()
    for i in range(7, 10):
        weights[i].wait()
    rows_in = [
        flat_slots(arrived[i].reshape(n_ep, capacity, share)) for i in range(n_tp)
    ]
    residual = (jnp.concatenate(rows_in, axis=1) + projected).astype(BF16).astype(F32)
    flat = rms(residual, ffn_gain[...]).astype(BF16)
    act = (jax.nn.silu(mm(flat, eg[...])) * mm(flat, eu[...])).astype(BF16)
    result = mm(act, ed[...])
    for e in range(n_ep):
        for t in range(n_tp):
            computed[e * n_tp + t] = result[
                e * capacity : (e + 1) * capacity, t * share : (t + 1) * share
            ].astype(BF16)
    returned[me] = computed[me]

    for other_ep, other_tp in peers:
        remote(
            computed.at[other_ep * n_tp + other_tp], returned.at[me], back_sem, other_ep, other_tp
        ).start()
    total = resid[tp] + share_out[tp].astype(F32)
    whole(share_out, share_in, share_sem, n_tp - 1).wait_recv()
    for i in range(n_tp - 1):
        total = total + share_in[i].astype(F32)
    whole(heads, heads, head_sem, n_tp - 1).wait_send()
    whole(share_out, share_in, share_sem, n_tp - 1).wait_send()
    whole(head_rows, head_slots, slot_sem, n_dev - 1).wait_send()
    whole(relay, relay, relay_sem, n_hi - 1).wait_send()
    remote(relayed_all, relayed_all, disp_sem, ep, lax.rem(tp + 1, n_tp)).wait_send()
    whole(computed, returned, back_sem, n_dev - 1).wait_recv()
    back = flat_slots(returned[...]).astype(BF16)
    routed = mm(mix_high, back) + mm(mix_low, back)
    out[...] = (total + routed).astype(BF16)

    whole(computed, returned, back_sem, n_dev - 1).wait_send()


def shards(
    n_ep,
    n_tp,
    tokens,
    kv_cache,
    lengths,
    attn_gain,
    w_query,
    w_key,
    w_value,
    lambdas,
    head_gain,
    w_out,
    ffn_gain,
    w_shared_gate,
    w_shared_up,
    w_shared_down,
    routing,
    route_weights,
    w_exp_gate,
    w_exp_up,
    w_exp_down,
):
    seqs, width = tokens.shape
    lanes = kv_cache.shape[2]
    v_width = head_gain.shape[0]
    per_kv = lambdas.shape[0]
    n_dev = n_ep * n_tp
    capacity = max(2, 2 * seqs * routing.shape[1] // (w_exp_gate.shape[0] * n_dev))
    share = width // n_tp
    n_lo = 2 if n_ep % 2 == 0 else 1
    n_hi = n_ep // n_lo
    plane = n_lo * n_tp
    side = lanes // v_width * 2
    packs = seqs // side
    rows = seqs * per_kv
    fold = side * v_width
    group = next(g for g in (4, 2, 1) if packs % g == 0)
    small = [
        lengths,
        lambdas,
        tokens,
        attn_gain[None, :],
        head_gain[None, :],
        ffn_gain[None, :],
        routing.T,
        route_weights.T,
    ]
    big = [
        kv_cache,
        w_query,
        w_key.T,
        w_value.T,
        w_out,
        w_shared_gate,
        w_shared_up,
        w_shared_down,
        w_exp_gate,
        w_exp_up,
        w_exp_down,
    ]
    held = [pltpu.SMEM(x.shape, x.dtype) for x in small[:2]]
    held += [pltpu.VMEM(x.shape, x.dtype) for x in small[2:]]
    held += [pltpu.VMEM(x.shape, BF16) for x in big[:8]]
    held += [pltpu.VMEM(x.shape[1:], BF16) for x in big[8:]]
    vmem = pl.BlockSpec(memory_space=pltpu.VMEM)
    dma = pltpu.SemaphoreType.DMA
    return pl.pallas_call(
        functools.partial(layer, n_ep, n_tp, capacity, group),
        out_shape=pltpu.VMEM((seqs, share), BF16),
        in_specs=[pl.BlockSpec(memory_space=pltpu.HBM)] * (len(small) + len(big)),
        out_specs=vmem,
        scratch_shapes=held
        + [
            pltpu.VMEM((2 * rows, fold), BF16),
            pltpu.VMEM((2 * rows, lanes), F32),
            pltpu.VMEM((rows, fold), F32),
            pltpu.VMEM((rows, fold), F32),
            pltpu.VMEM((n_tp, seqs, per_kv * v_width), BF16),
            pltpu.VMEM((n_dev, capacity, per_kv * v_width), BF16),
            pltpu.VMEM((n_dev, capacity, per_kv * v_width), BF16),
            pltpu.VMEM((n_tp, seqs, share), F32),
            pltpu.VMEM((n_hi, seqs, plane * capacity), BF16),
            pltpu.VMEM((n_hi, seqs, share), BF16),
            pltpu.VMEM((n_hi, plane, capacity, share), BF16),
            pltpu.VMEM((n_tp, n_hi, n_lo, capacity, share), BF16),
            pltpu.VMEM((n_dev, capacity, share), BF16),
            pltpu.VMEM((n_dev, capacity, share), BF16),
            pltpu.VMEM((n_tp, seqs, share), BF16),
            pltpu.VMEM((n_tp, seqs, share), BF16),
            dma((len(small),)),
            dma((packs,)),
            dma((10,)),
            dma((2,)),
            dma((2,)),
            dma((1 + n_hi,)),
            dma((2,)),
            dma((2,)),
            dma((2,)),
        ],
        compiler_params=pltpu.CompilerParams(
            collective_id=0, has_side_effects=True, vmem_limit_bytes=60 * 1024 * 1024
        ),
    )(
        *small,
        *big,
    )


def solution(mesh):
    return jax.shard_map(
        functools.partial(shards, mesh.shape["ep"], mesh.shape["tp"]),
        mesh=mesh,
        in_specs=(
            P("ep", None),
            P("ep", None, "tp"),
            P("ep"),
            P(),
            P(None, "tp"),
            P(None, "tp"),
            P(None, "tp"),
            P("tp"),
            P(),
            P(),
            P(),
            P(None, "tp"),
            P(None, "tp"),
            P("tp", None),
            P(),
            P("ep", None),
            P(("ep", "tp"), None, None),
            P(("ep", "tp"), None, None),
            P(("ep", "tp"), None, None),
        ),
        out_specs=P("ep", "tp"),
        check_vma=False,
    )
```

```python
import functools

import jax
import jax.numpy as jnp
from jax import lax
from jax.experimental import pallas as pl
from jax.experimental.pallas import tpu as pltpu
from jax.sharding import PartitionSpec as P

epsilon = 1e-06
neg_fill = -1e30
MESH = pl.DeviceIdType.MESH
F32 = jnp.float32
BF16 = jnp.bfloat16


def mm(left, right):
    return jnp.dot(left, right, preferred_element_type=F32)


def iota(shape, dim):
    return lax.broadcasted_iota(jnp.int32, shape, dim)


def hot(condition):
    return condition.astype(F32).astype(BF16)


def mm_t(left, right):
    return lax.dot_general(left, right, (((1,), (1,)), ((), ())), preferred_element_type=F32)


def exact(left, right, last):
    return lax.dot_general(
        left,
        right,
        (((1,), (last,)), ((), ())),
        preferred_element_type=F32,
        precision=lax.Precision.HIGHEST,
    )


def rms(values, gain):
    return values * lax.rsqrt(jnp.mean(values * values, axis=-1, keepdims=True) + epsilon) * gain


def flat_slots(values):
    blocks, rows, width = values.shape
    wide = values.astype(F32)
    if rows % 8 == 0:
        return wide.reshape(blocks * rows, width)
    return jnp.concatenate([wide[i] for i in range(blocks)], axis=0)


def layer(
    n_ep,
    n_tp,
    capacity,
    group,
    lengths_hbm,
    lambdas_hbm,
    tokens_hbm,
    attn_gain_hbm,
    head_gain_hbm,
    ffn_gain_hbm,
    routing_hbm,
    route_weights_hbm,
    kv_hbm,
    wq_hbm,
    wk_hbm,
    wv_hbm,
    wo_hbm,
    sg_hbm,
    su_hbm,
    sd_hbm,
    eg_hbm,
    eu_hbm,
    ed_hbm,
    out,
    lengths,
    lambdas,
    tokens,
    attn_gain,
    head_gain,
    ffn_gain,
    routing,
    route_weights,
    kv,
    wq,
    wk,
    wv,
    wo,
    sg,
    su,
    sd,
    eg,
    eu,
    ed,
    q_rows,
    score_new,
    value_new,
    mix_rows,
    heads,
    head_rows,
    head_slots,
    resid,
    relay_pick,
    relay,
    packed,
    arrived,
    computed,
    returned,
    share_out,
    share_in,
    in_sem,
    kv_sem,
    w_sem,
    head_sem,
    slot_sem,
    relay_sem,
    disp_sem,
    back_sem,
    share_sem,
):
    n_dev = n_ep * n_tp
    ep = lax.axis_index("ep")
    tp = lax.axis_index("tp")
    me = ep * n_tp + tp
    n_hi, plane = packed.shape[:2]
    n_lo = n_ep // n_hi
    hi = ep // n_lo
    lo = lax.rem(ep, n_lo)
    spot_in_plane = lo * n_tp + tp
    seqs, width = tokens.shape
    cache_len, lanes = kv.shape[1], kv.shape[2]
    v_width = lanes // 2
    qk_width = v_width // 2
    per_kv = lambdas.shape[0]
    side = lanes // v_width * 2
    packs = seqs // side
    half = side * per_kv
    block = 2 * half
    share = width // n_tp
    scaling = qk_width**-0.5
    barrier = pltpu.get_barrier_semaphore()

    inputs = [
        pltpu.make_async_copy(source, target, in_sem.at[i])
        for i, (source, target) in enumerate(
            [
                (tokens_hbm, tokens),
                (attn_gain_hbm, attn_gain),
                (routing_hbm, routing),
                (route_weights_hbm, route_weights),
                (head_gain_hbm, head_gain),
                (lambdas_hbm, lambdas),
                (lengths_hbm, lengths),
                (ffn_gain_hbm, ffn_gain),
            ]
        )
    ]
    weights = [
        pltpu.make_async_copy(src, dst, w_sem.at[i])
        for i, (src, dst) in enumerate(
            [
                (wq_hbm, wq),
                (wk_hbm, wk),
                (wv_hbm, wv),
                (wo_hbm, wo),
                (sg_hbm, sg),
                (su_hbm, su),
                (sd_hbm, sd),
                (eg_hbm.at[0], eg),
                (eu_hbm.at[0], eu),
                (ed_hbm.at[0], ed),
            ]
        )
    ]

    def kv_copy(pack):
        rows = pl.ds(side * pack, side)
        return pltpu.make_async_copy(kv_hbm.at[rows], kv.at[rows], kv_sem.at[pack])

    inputs[0].start()
    inputs[1].start()
    for i in range(3):
        weights[i].start()
    for i in range(2, 8):
        inputs[i].start()

    for step in range(1, n_dev):
        other = lax.rem(me + step, n_dev)
        pl.semaphore_signal(
            barrier, inc=1, device_id=(other // n_tp, lax.rem(other, n_tp)), device_id_type=MESH
        )

    def start_kv(pack, carry):
        kv_copy(pack).start()
        return carry

    lax.fori_loop(0, packs, start_kv, 0)

    def remote(source, target, sem, other_ep, other_tp):
        return pltpu.make_async_remote_copy(
            src_ref=source,
            dst_ref=target,
            send_sem=sem.at[0],
            recv_sem=sem.at[1],
            device_id=(other_ep, other_tp),
            device_id_type=MESH,
        )

    def whole(source, target, sem, count):
        part = pl.ds(0, count)
        return remote(
            source.at[part], target.at[part], sem, lax.rem(ep + 1, n_ep), lax.rem(tp + 1, n_tp)
        )

    def far_first(step, mine, count):
        late = 2 * mine // count
        up = count - 1 - step
        up = up - (mine >= up).astype(jnp.int32)
        down = step + (step >= mine).astype(jnp.int32)
        return (1 - late) * up + late * down

    peers = [
        (far_first(k, ep, n_ep), lax.rem(tp + t, n_tp))
        for k in range(n_ep - 1)
        for t in range(n_tp)
    ]
    peers += [(ep, lax.rem(tp + t, n_tp)) for t in range(1, n_tp)]
    half_planes = n_hi // 2 if n_hi % 2 == 0 else n_hi
    upper = hi // half_planes
    near_planes = [
        upper * half_planes + lax.rem(hi + k, half_planes) for k in range(1, half_planes)
    ]
    across = n_hi // half_planes - 1
    far_planes = [
        half_planes - upper + k * (1 - 2 * upper) for k in range(across * half_planes)
    ]

    def relay_copy(source, target):
        return pltpu.make_async_remote_copy(
            src_ref=tokens.at[:, pl.ds(pl.multiple_of(tp * share, share), share)],
            dst_ref=relay.at[source],
            send_sem=relay_sem.at[0],
            recv_sem=relay_sem.at[1 + source],
            device_id=(target * n_lo + lo, tp),
            device_id_type=MESH,
        )

    for i in range(2):
        inputs[i].wait()
    normed = rms(tokens[...].astype(F32), attn_gain[...]).astype(BF16)
    for i in range(2, 4):
        inputs[i].wait()
    top_count, batch = routing.shape

    def lookup(select, table):
        if n_dev > 256:
            return exact(select, table, 1)
        return mm_t(select.astype(BF16), table.astype(BF16))

    picked = (iota((seqs, batch), 0) + ep * seqs == iota((seqs, batch), 1)).astype(F32)
    ids = routing[...].astype(F32)
    own_ids = lookup(picked, ids).astype(jnp.int32)
    high = route_weights[...].astype(BF16)
    low = (route_weights[...] - high.astype(F32)).astype(BF16)
    same = hot(iota((seqs, seqs), 0) == iota((seqs, seqs), 1))
    own_weights = mm_t(same, high) + mm_t(same, low)
    before = hot(iota((seqs, seqs), 1) < iota((seqs, seqs), 0))

    def slots(count, expert_of):
        column = iota((seqs, count), 1)
        expert = expert_of(column // capacity)
        named = [own_ids[:, k : k + 1] == expert for k in range(top_count)]
        hit = functools.reduce(jnp.logical_or, named)
        rank = mm(before, hot(hit))
        chosen = hit & (rank == lax.rem(column, capacity).astype(F32))
        return named, chosen

    named_all, chosen_all = slots(n_dev * capacity, lambda expert: expert)
    mixing = jnp.zeros((seqs, n_dev * capacity), F32)
    for k in range(top_count):
        mixing = mixing + jnp.where(named_all[k] & chosen_all, own_weights[:, k : k + 1], 0.0)
    row = iota((seqs * per_kv, seqs), 0)
    repeat = hot(row // per_kv == iota((seqs * per_kv, seqs), 1))
    row_choice = mm(repeat, hot(chosen_all)).astype(BF16)
    relayed = n_hi * seqs
    row = iota((relayed, batch), 0)
    picked = (row // seqs * n_lo + lo) * seqs + lax.rem(row, seqs) == iota((relayed, batch), 1)
    relay_ids = lookup(picked.astype(F32), ids).astype(jnp.int32)
    column = iota((relayed, plane * capacity), 1)
    expert = hi * plane + column // capacity
    hit = functools.reduce(
        jnp.logical_or, [relay_ids[:, k : k + 1] == expert for k in range(top_count)]
    )
    row, other = iota((relayed, relayed), 0), iota((relayed, relayed), 1)
    earlier = hot((row // seqs == other // seqs) & (other < row))
    chosen = hit & (mm(earlier, hot(hit)) == lax.rem(column, capacity).astype(F32))
    chosen = hot(chosen)
    for i in range(n_hi):
        relay_pick[i] = chosen[i * seqs : (i + 1) * seqs, :]
    mix_high = mixing.astype(BF16)
    mix_low = (mixing - mix_high.astype(F32)).astype(BF16)

    for i in range(3):
        weights[i].wait()
    queries = mm(normed, wq[...]).astype(BF16)
    key_new = mm_t(normed, wk[...]).astype(BF16)
    val_new = mm_t(normed, wv[...]).astype(BF16)
    fold_width = side * v_width
    spot = (v_width, fold_width)
    tile = hot(iota(spot, 0) == lax.rem(iota(spot, 1), v_width))

    rows = seqs * 2 * per_kv
    row = iota((rows, seqs), 0)
    spread = hot(row // block * side + lax.rem(row, half) // per_kv == iota((rows, seqs), 1))
    wide_q = mm(spread, queries)
    row = iota(wide_q.shape, 0)
    lane = iota(wide_q.shape, 1)
    mine = (lane // v_width == lax.rem(row, per_kv)) & (
        lax.rem(lane, v_width) // qk_width == lax.rem(row, block) // half
    )
    wide_q = jnp.where(mine, wide_q, 0.0).astype(BF16)
    fold = (queries.shape[1], fold_width)
    folded = mm(wide_q, hot(lax.rem(iota(fold, 0), v_width) == lax.rem(iota(fold, 1), v_width)))
    row = iota(folded.shape, 0)
    lane = iota(folded.shape, 1)
    folded = jnp.where(lax.rem(row, half) // per_kv == lane // v_width, folded, 0.0)
    q_rows[...] = folded.astype(BF16)
    keys_wide = mm(spread, mm(key_new, tile).astype(BF16))
    fresh = jnp.sum(folded * keys_wide, axis=1, keepdims=True)
    score_new[...] = jnp.broadcast_to(fresh, score_new.shape)
    value_new[...] = mm(repeat, mm(val_new, tile).astype(BF16))

    for i in range(4, 8):
        inputs[i].wait()
    wide_gain = jnp.concatenate([head_gain[...]] * side, axis=1)
    row = iota((block, 1), 0)
    factor = jnp.ones((block, 1), F32)
    for g in range(per_kv):
        factor = jnp.where((row >= half) & (lax.rem(row, per_kv) == g), lambdas[g], factor)

    for i in range(3, 10):
        weights[i].start()

    def attend(index, carry):
        first = index * group
        for i in range(group):
            kv_copy(first + i).wait()
        stage = []
        values = []
        for i in range(group):
            pack = first + i
            keys = []
            swapped = []
            for j in range(0, side, 2):
                even = kv[side * pack + j]
                odd = pltpu.roll(kv[side * pack + j + 1], v_width, 1)
                keys += [even[:, :v_width], odd[:, v_width:]]
                swapped += [odd[:, :v_width], even[:, v_width:]]
            keys = jnp.concatenate(keys, axis=1)
            values.append(jnp.concatenate(swapped, axis=1))
            query = q_rows[pl.ds(pl.multiple_of(pack * block, block), block), :]
            stage.append(mm_t(query, keys))
        weighed = []
        for i in range(group):
            pack = first + i
            fresh = score_new[pl.ds(pl.multiple_of(pack * block, block), block), :][:, :1]
            owner = lax.rem(iota((block, 1), 0), half) // per_kv
            limit = jnp.zeros((block, 1), jnp.int32)
            for j in range(side):
                limit = jnp.where(owner == j, lengths[side * pack + j], limit)
            valid = iota((block, cache_len), 1) < limit
            scores = jnp.where(valid, stage[i], neg_fill)
            highest = jnp.maximum(jnp.max(scores, axis=1, keepdims=True), fresh)
            expo = jnp.exp((scores - highest) * scaling)
            expo_new = jnp.exp((fresh - highest) * scaling)
            scale = factor / (jnp.sum(expo, axis=1, keepdims=True) + expo_new)
            expo = expo * scale
            expo_new = expo_new * scale
            weighed.append(
                (
                    (expo[:half] - expo[half:]).astype(BF16),
                    (expo_new[:half] - expo_new[half:]).astype(BF16).astype(F32),
                )
            )
        for i in range(group):
            pack = first + i
            spots = pl.ds(pl.multiple_of(pack * half, half), half)
            mixed = mm(weighed[i][0], values[i]) + weighed[i][1] * value_new[spots, :]
            owner = iota(mixed.shape, 0) // per_kv
            own = owner + 1 - 2 * lax.rem(owner, 2) == iota(mixed.shape, 1) // v_width
            mix_rows[spots, :] = jnp.where(own, mixed, 0.0)
        return carry

    def open_links():
        pl.semaphore_wait(barrier, n_dev - 1)
        outer = (hi != half_planes - 1 + upper).astype(jnp.int32)
        for k in range(len(far_planes)):
            k = k + outer * (half_planes - 1 - 2 * k)
            relay_copy(hi, half_planes - upper + k * (1 - 2 * upper)).start()
        for other in near_planes:
            relay_copy(hi, other).start()

    first_part = packs // group // 2
    pl.when(hi == n_hi - 1)(open_links)
    lax.fori_loop(0, first_part, attend, 0)
    pl.when((me >= 2) & (hi < n_hi - 1))(open_links)
    lax.fori_loop(first_part, packs // group, attend, 0)
    pl.when(me < 2)(open_links)

    mixed = mix_rows[...]
    mean = jnp.sum(mixed * mixed, axis=1, keepdims=True) * (1.0 / v_width)
    head_out = (mixed * lax.rsqrt(mean + epsilon) * wide_gain).astype(BF16)
    unfold = (fold_width, per_kv * v_width)
    shifted = hot(lax.rem(iota(unfold, 1), v_width) == lax.rem(iota(unfold, 0), v_width))
    laid = mm(head_out, shifted)
    own = iota(laid.shape, 1) // v_width == lax.rem(iota(laid.shape, 0), per_kv)
    laid = jnp.where(own, laid, 0.0).astype(BF16)
    gather = (seqs, seqs * per_kv)
    heads[tp] = mm(hot(iota(gather, 1) // per_kv == iota(gather, 0)), laid).astype(BF16)

    for t in range(1, n_tp):
        remote(heads.at[tp], heads.at[tp], head_sem, ep, lax.rem(tp + t, n_tp)).start()
    picked_rows = lax.dot_general(
        row_choice, laid, (((0,), (0,)), ((), ())), preferred_element_type=F32
    )
    for e in range(n_dev):
        head_rows[e] = picked_rows[e * capacity : (e + 1) * capacity, :].astype(BF16)
    head_slots[tp * n_ep + ep] = head_rows[me]
    for other_ep, other_tp in peers:
        remote(
            head_rows.at[other_ep * n_tp + other_tp],
            head_slots.at[tp * n_ep + ep],
            slot_sem,
            other_ep,
            other_tp,
        ).start()
    relay[hi] = tokens[:, pl.ds(pl.multiple_of(tp * share, share), share)]
    for index, source in enumerate([hi] + near_planes + far_planes):
        if index:
            relay_copy(source, lax.rem(hi + 1, n_hi)).wait_recv()
        rows_out = lax.dot_general(
            relay_pick[source], relay[source], (((0,), (0,)), ((), ())), preferred_element_type=F32
        )
        for q in range(plane):
            packed[source, q] = rows_out[q * capacity : (q + 1) * capacity, :].astype(BF16)
        arrived[tp, source, lo] = packed[source, spot_in_plane]
        for q in range(1, plane):
            other = lax.rem(spot_in_plane + q, plane)
            remote(
                packed.at[source, other],
                arrived.at[tp, source, lo],
                disp_sem,
                hi * n_lo + other // n_tp,
                lax.rem(other, n_tp),
            ).start()
    weights[3].wait()
    whole(heads, heads, head_sem, n_tp - 1).wait_recv()
    depth = heads.shape[2]
    projected = jnp.zeros((seqs, width), F32)
    for i in range(n_tp):
        piece = mm(heads[i], wo[i * depth : (i + 1) * depth, :])
        projected = projected + piece.astype(BF16).astype(F32)
    residual = (tokens[...].astype(F32) + projected).astype(BF16).astype(F32)
    for i in range(n_tp):
        resid[i] = residual[:, i * share : (i + 1) * share]
    ffn_in = rms(residual, ffn_gain[...]).astype(BF16)

    for i in range(4, 7):
        weights[i].wait()
    shared_act = (jax.nn.silu(mm(ffn_in, sg[...])) * mm(ffn_in, su[...])).astype(BF16)
    shared_part = mm(shared_act, sd[...])
    for i in range(n_tp):
        share_out[i] = shared_part[:, i * share : (i + 1) * share].astype(BF16)

    for t in range(1, n_tp):
        other = lax.rem(tp + t, n_tp)
        remote(share_out.at[other], share_in.at[t - 1], share_sem, ep, other).start()

    whole(head_rows, head_slots, slot_sem, n_dev - 1).wait_recv()
    projected = jnp.zeros((n_ep * capacity, width), F32)
    for i in range(n_tp):
        piece = flat_slots(head_slots[i * n_ep : (i + 1) * n_ep]).astype(BF16)
        piece = mm(piece, wo[i * depth : (i + 1) * depth, :])
        projected = projected + piece.astype(BF16).astype(F32)
    relayed_all = packed.at[:, pl.ds(0, plane - 1)]
    remote(relayed_all, relayed_all, disp_sem, ep, lax.rem(tp + 1, n_tp)).wait_recv()
    for i in range(7, 10):
        weights[i].wait()
    rows_in = [
        flat_slots(arrived[i].reshape(n_ep, capacity, share)) for i in range(n_tp)
    ]
    residual = (jnp.concatenate(rows_in, axis=1) + projected).astype(BF16).astype(F32)
    flat = rms(residual, ffn_gain[...]).astype(BF16)
    act = (jax.nn.silu(mm(flat, eg[...])) * mm(flat, eu[...])).astype(BF16)
    result = mm(act, ed[...])
    for e in range(n_ep):
        for t in range(n_tp):
            computed[e * n_tp + t] = result[
                e * capacity : (e + 1) * capacity, t * share : (t + 1) * share
            ].astype(BF16)
    returned[me] = computed[me]
    for other_ep, other_tp in peers:
        remote(
            computed.at[other_ep * n_tp + other_tp], returned.at[me], back_sem, other_ep, other_tp
        ).start()
    total = resid[tp] + share_out[tp].astype(F32)
    whole(share_out, share_in, share_sem, n_tp - 1).wait_recv()
    for i in range(n_tp - 1):
        total = total + share_in[i].astype(F32)
    whole(heads, heads, head_sem, n_tp - 1).wait_send()
    whole(share_out, share_in, share_sem, n_tp - 1).wait_send()
    whole(head_rows, head_slots, slot_sem, n_dev - 1).wait_send()
    whole(relay, relay, relay_sem, n_hi - 1).wait_send()
    remote(relayed_all, relayed_all, disp_sem, ep, lax.rem(tp + 1, n_tp)).wait_send()
    whole(computed, returned, back_sem, n_dev - 1).wait_recv()
    back = flat_slots(returned[...]).astype(BF16)
    routed = mm(mix_high, back) + mm(mix_low, back)
    out[...] = (total + routed).astype(BF16)

    whole(computed, returned, back_sem, n_dev - 1).wait_send()


def shards(
    n_ep,
    n_tp,
    tokens,
    kv_cache,
    lengths,
    attn_gain,
    w_query,
    w_key,
    w_value,
    lambdas,
    head_gain,
    w_out,
    ffn_gain,
    w_shared_gate,
    w_shared_up,
    w_shared_down,
    routing,
    route_weights,
    w_exp_gate,
    w_exp_up,
    w_exp_down,
):
    seqs, width = tokens.shape
    lanes = kv_cache.shape[2]
    v_width = head_gain.shape[0]
    per_kv = lambdas.shape[0]
    n_dev = n_ep * n_tp
    capacity = max(2, 2 * seqs * routing.shape[1] // (w_exp_gate.shape[0] * n_dev))
    share = width // n_tp
    n_lo = 2 if n_ep % 2 == 0 else 1
    n_hi = n_ep // n_lo
    plane = n_lo * n_tp
    side = lanes // v_width * 2
    packs = seqs // side
    rows = seqs * per_kv
    fold = side * v_width
    group = next(g for g in (4, 2, 1) if packs % g == 0)
    small = [
        lengths,
        lambdas,
        tokens,
        attn_gain[None, :],
        head_gain[None, :],
        ffn_gain[None, :],
        routing.T,
        route_weights.T,
    ]
    big = [
        kv_cache,
        w_query,
        w_key.T,
        w_value.T,
        w_out,
        w_shared_gate,
        w_shared_up,
        w_shared_down,
        w_exp_gate,
        w_exp_up,
        w_exp_down,
    ]
    held = [pltpu.SMEM(x.shape, x.dtype) for x in small[:2]]
    held += [pltpu.VMEM(x.shape, x.dtype) for x in small[2:]]
    held += [pltpu.VMEM(x.shape, BF16) for x in big[:8]]
    held += [pltpu.VMEM(x.shape[1:], BF16) for x in big[8:]]
    vmem = pl.BlockSpec(memory_space=pltpu.VMEM)
    dma = pltpu.SemaphoreType.DMA
    return pl.pallas_call(
        functools.partial(layer, n_ep, n_tp, capacity, group),
        out_shape=pltpu.VMEM((seqs, share), BF16),
        in_specs=[pl.BlockSpec(memory_space=pltpu.HBM)] * (len(small) + len(big)),
        out_specs=vmem,
        scratch_shapes=held
        + [
            pltpu.VMEM((2 * rows, fold), BF16),
            pltpu.VMEM((2 * rows, lanes), F32),
            pltpu.VMEM((rows, fold), F32),
            pltpu.VMEM((rows, fold), F32),
            pltpu.VMEM((n_tp, seqs, per_kv * v_width), BF16),
            pltpu.VMEM((n_dev, capacity, per_kv * v_width), BF16),
            pltpu.VMEM((n_dev, capacity, per_kv * v_width), BF16),
            pltpu.VMEM((n_tp, seqs, share), F32),
            pltpu.VMEM((n_hi, seqs, plane * capacity), BF16),
            pltpu.VMEM((n_hi, seqs, share), BF16),
            pltpu.VMEM((n_hi, plane, capacity, share), BF16),
            pltpu.VMEM((n_tp, n_hi, n_lo, capacity, share), BF16),
            pltpu.VMEM((n_dev, capacity, share), BF16),
            pltpu.VMEM((n_dev, capacity, share), BF16),
            pltpu.VMEM((n_tp, seqs, share), BF16),
            pltpu.VMEM((n_tp, seqs, share), BF16),
            dma((len(small),)),
            dma((packs,)),
            dma((10,)),
            dma((2,)),
            dma((2,)),
            dma((1 + n_hi,)),
            dma((2,)),
            dma((2,)),
            dma((2,)),
        ],
        compiler_params=pltpu.CompilerParams(
            collective_id=0, has_side_effects=True, vmem_limit_bytes=60 * 1024 * 1024
        ),
    )(
        *small,
        *big,
    )


def solution(mesh):
    return jax.shard_map(
        functools.partial(shards, mesh.shape["ep"], mesh.shape["tp"]),
        mesh=mesh,
        in_specs=(
            P("ep", None),
            P("ep", None, "tp"),
            P("ep"),
            P(),
            P(None, "tp"),
            P(None, "tp"),
            P(None, "tp"),
            P("tp"),
            P(),
            P(),
            P(),
            P(None, "tp"),
            P(None, "tp"),
            P("tp", None),
            P(),
            P("ep", None),
            P(("ep", "tp"), None, None),
            P(("ep", "tp"), None, None),
            P(("ep", "tp"), None, None),
        ),
        out_specs=P("ep", "tp"),
        check_vma=False,
    )
```

```python
import functools

import jax
import jax.numpy as jnp
from jax import lax
from jax.experimental import pallas as pl
from jax.experimental.pallas import tpu as pltpu
from jax.sharding import PartitionSpec as P

epsilon = 1e-06
neg_fill = -1e30
MESH = pl.DeviceIdType.MESH
F32 = jnp.float32
BF16 = jnp.bfloat16


def mm(left, right):
    return jnp.dot(left, right, preferred_element_type=F32)


def iota(shape, dim):
    return lax.broadcasted_iota(jnp.int32, shape, dim)


def hot(condition):
    return condition.astype(F32).astype(BF16)


def mm_t(left, right):
    return lax.dot_general(left, right, (((1,), (1,)), ((), ())), preferred_element_type=F32)


def exact(left, right, last):
    return lax.dot_general(
        left,
        right,
        (((1,), (last,)), ((), ())),
        preferred_element_type=F32,
        precision=lax.Precision.HIGHEST,
    )


def rms(values, gain):
    return values * lax.rsqrt(jnp.mean(values * values, axis=-1, keepdims=True) + epsilon) * gain


def flat_slots(values):
    blocks, rows, width = values.shape
    wide = values.astype(F32)
    if rows % 8 == 0:
        return wide.reshape(blocks * rows, width)
    return jnp.concatenate([wide[i] for i in range(blocks)], axis=0)


def layer(
    n_ep,
    n_tp,
    capacity,
    group,
    lengths_hbm,
    lambdas_hbm,
    tokens_hbm,
    attn_gain_hbm,
    head_gain_hbm,
    ffn_gain_hbm,
    routing_hbm,
    route_weights_hbm,
    kv_hbm,
    wq_hbm,
    wk_hbm,
    wv_hbm,
    wo_hbm,
    sg_hbm,
    su_hbm,
    sd_hbm,
    eg_hbm,
    eu_hbm,
    ed_hbm,
    out,
    lengths,
    lambdas,
    tokens,
    attn_gain,
    head_gain,
    ffn_gain,
    routing,
    route_weights,
    kv,
    wq,
    wk,
    wv,
    wo,
    sg,
    su,
    sd,
    eg,
    eu,
    ed,
    q_rows,
    score_new,
    value_new,
    mix_rows,
    heads,
    head_rows,
    head_slots,
    resid,
    relay_pick,
    relay,
    packed,
    arrived,
    computed,
    returned,
    share_out,
    share_in,
    in_sem,
    kv_sem,
    w_sem,
    head_sem,
    slot_sem,
    relay_sem,
    disp_sem,
    back_sem,
    share_sem,
):
    n_dev = n_ep * n_tp
    ep = lax.axis_index("ep")
    tp = lax.axis_index("tp")
    me = ep * n_tp + tp
    n_hi, plane = packed.shape[:2]
    n_lo = n_ep // n_hi
    hi = ep // n_lo
    lo = lax.rem(ep, n_lo)
    spot_in_plane = lo * n_tp + tp
    seqs, width = tokens.shape
    cache_len, lanes = kv.shape[1], kv.shape[2]
    v_width = lanes // 2
    qk_width = v_width // 2
    per_kv = lambdas.shape[0]
    side = lanes // v_width * 2
    packs = seqs // side
    half = side * per_kv
    block = 2 * half
    share = width // n_tp
    scaling = qk_width**-0.5
    barrier = pltpu.get_barrier_semaphore()

    inputs = [
        pltpu.make_async_copy(source, target, in_sem.at[i])
        for i, (source, target) in enumerate(
            [
                (tokens_hbm, tokens),
                (attn_gain_hbm, attn_gain),
                (routing_hbm, routing),
                (route_weights_hbm, route_weights),
                (head_gain_hbm, head_gain),
                (lambdas_hbm, lambdas),
                (lengths_hbm, lengths),
                (ffn_gain_hbm, ffn_gain),
            ]
        )
    ]
    weights = [
        pltpu.make_async_copy(src, dst, w_sem.at[i])
        for i, (src, dst) in enumerate(
            [
                (wq_hbm, wq),
                (wk_hbm, wk),
                (wv_hbm, wv),
                (wo_hbm, wo),
                (sg_hbm, sg),
                (su_hbm, su),
                (sd_hbm, sd),
                (eg_hbm.at[0], eg),
                (eu_hbm.at[0], eu),
                (ed_hbm.at[0], ed),
            ]
        )
    ]

    def kv_copy(pack):
        rows = pl.ds(side * pack, side)
        return pltpu.make_async_copy(kv_hbm.at[rows], kv.at[rows], kv_sem.at[pack])

    inputs[0].start()
    inputs[1].start()
    for i in range(3):
        weights[i].start()
    for i in range(2, 8):
        inputs[i].start()

    for step in range(1, n_dev):
        other = lax.rem(me + step, n_dev)
        pl.semaphore_signal(
            barrier, inc=1, device_id=(other // n_tp, lax.rem(other, n_tp)), device_id_type=MESH
        )

    def start_kv(pack, carry):
        kv_copy(pack).start()
        return carry

    lax.fori_loop(0, packs, start_kv, 0)

    def remote(source, target, sem, other_ep, other_tp):
        return pltpu.make_async_remote_copy(
            src_ref=source,
            dst_ref=target,
            send_sem=sem.at[0],
            recv_sem=sem.at[1],
            device_id=(other_ep, other_tp),
            device_id_type=MESH,
        )

    def whole(source, target, sem, count):
        part = pl.ds(0, count)
        return remote(
            source.at[part], target.at[part], sem, lax.rem(ep + 1, n_ep), lax.rem(tp + 1, n_tp)
        )

    def far_first(step, mine, count):
        late = 2 * mine // count
        up = count - 1 - step
        up = up - (mine >= up).astype(jnp.int32)
        down = step + (step >= mine).astype(jnp.int32)
        return (1 - late) * up + late * down

    peers = [
        (far_first(k, ep, n_ep), lax.rem(tp + t, n_tp))
        for k in range(n_ep - 1)
        for t in range(n_tp)
    ]
    peers += [(ep, lax.rem(tp + t, n_tp)) for t in range(1, n_tp)]
    half_planes = n_hi // 2 if n_hi % 2 == 0 else n_hi
    upper = hi // half_planes
    near_planes = [
        upper * half_planes + lax.rem(hi + k, half_planes) for k in range(1, half_planes)
    ]
    across = n_hi // half_planes - 1
    far_planes = [
        half_planes - upper + k * (1 - 2 * upper) for k in range(across * half_planes)
    ]

    def relay_copy(source, target):
        return pltpu.make_async_remote_copy(
            src_ref=tokens.at[:, pl.ds(pl.multiple_of(tp * share, share), share)],
            dst_ref=relay.at[source],
            send_sem=relay_sem.at[0],
            recv_sem=relay_sem.at[1 + source],
            device_id=(target * n_lo + lo, tp),
            device_id_type=MESH,
        )

    for i in range(2):
        inputs[i].wait()
    normed = rms(tokens[...].astype(F32), attn_gain[...]).astype(BF16)
    for i in range(2, 4):
        inputs[i].wait()
    top_count, batch = routing.shape

    def lookup(select, table):
        if n_dev > 256:
            return exact(select, table, 1)
        return mm_t(select.astype(BF16), table.astype(BF16))

    picked = (iota((seqs, batch), 0) + ep * seqs == iota((seqs, batch), 1)).astype(F32)
    ids = routing[...].astype(F32)
    own_ids = lookup(picked, ids).astype(jnp.int32)
    high = route_weights[...].astype(BF16)
    low = (route_weights[...] - high.astype(F32)).astype(BF16)
    same = hot(iota((seqs, seqs), 0) == iota((seqs, seqs), 1))
    own_weights = mm_t(same, high) + mm_t(same, low)
    before = hot(iota((seqs, seqs), 1) < iota((seqs, seqs), 0))

    def slots(count, expert_of):
        column = iota((seqs, count), 1)
        expert = expert_of(column // capacity)
        named = [own_ids[:, k : k + 1] == expert for k in range(top_count)]
        hit = functools.reduce(jnp.logical_or, named)
        rank = mm(before, hot(hit))
        chosen = hit & (rank == lax.rem(column, capacity).astype(F32))
        return named, chosen

    named_all, chosen_all = slots(n_dev * capacity, lambda expert: expert)
    mixing = jnp.zeros((seqs, n_dev * capacity), F32)
    for k in range(top_count):
        mixing = mixing + jnp.where(named_all[k] & chosen_all, own_weights[:, k : k + 1], 0.0)
    row = iota((seqs * per_kv, seqs), 0)
    repeat = hot(row // per_kv == iota((seqs * per_kv, seqs), 1))
    row_choice = mm(repeat, hot(chosen_all)).astype(BF16)
    relayed = n_hi * seqs
    row = iota((relayed, batch), 0)
    picked = (row // seqs * n_lo + lo) * seqs + lax.rem(row, seqs) == iota((relayed, batch), 1)
    relay_ids = lookup(picked.astype(F32), ids).astype(jnp.int32)
    column = iota((relayed, plane * capacity), 1)
    expert = hi * plane + column // capacity
    hit = functools.reduce(
        jnp.logical_or, [relay_ids[:, k : k + 1] == expert for k in range(top_count)]
    )
    row, other = iota((relayed, relayed), 0), iota((relayed, relayed), 1)
    earlier = hot((row // seqs == other // seqs) & (other < row))
    chosen = hit & (mm(earlier, hot(hit)) == lax.rem(column, capacity).astype(F32))
    chosen = hot(chosen)
    for i in range(n_hi):
        relay_pick[i] = chosen[i * seqs : (i + 1) * seqs, :]
    mix_high = mixing.astype(BF16)
    mix_low = (mixing - mix_high.astype(F32)).astype(BF16)

    for i in range(3):
        weights[i].wait()
    queries = mm(normed, wq[...]).astype(BF16)
    key_new = mm_t(normed, wk[...]).astype(BF16)
    val_new = mm_t(normed, wv[...]).astype(BF16)
    fold_width = side * v_width
    spot = (v_width, fold_width)
    tile = hot(iota(spot, 0) == lax.rem(iota(spot, 1), v_width))

    rows = seqs * 2 * per_kv
    row = iota((rows, seqs), 0)
    spread = hot(row // block * side + lax.rem(row, half) // per_kv == iota((rows, seqs), 1))
    wide_q = mm(spread, queries)
    row = iota(wide_q.shape, 0)
    lane = iota(wide_q.shape, 1)
    mine = (lane // v_width == lax.rem(row, per_kv)) & (
        lax.rem(lane, v_width) // qk_width == lax.rem(row, block) // half
    )
    wide_q = jnp.where(mine, wide_q, 0.0).astype(BF16)
    fold = (queries.shape[1], fold_width)
    folded = mm(wide_q, hot(lax.rem(iota(fold, 0), v_width) == lax.rem(iota(fold, 1), v_width)))
    row = iota(folded.shape, 0)
    lane = iota(folded.shape, 1)
    folded = jnp.where(lax.rem(row, half) // per_kv == lane // v_width, folded, 0.0)
    q_rows[...] = folded.astype(BF16)
    keys_wide = mm(spread, mm(key_new, tile).astype(BF16))
    fresh = jnp.sum(folded * keys_wide, axis=1, keepdims=True)
    score_new[...] = jnp.broadcast_to(fresh, score_new.shape)
    value_new[...] = mm(repeat, mm(val_new, tile).astype(BF16))

    for i in range(4, 8):
        inputs[i].wait()
    wide_gain = jnp.concatenate([head_gain[...]] * side, axis=1)
    row = iota((block, 1), 0)
    factor = jnp.ones((block, 1), F32)
    for g in range(per_kv):
        factor = jnp.where((row >= half) & (lax.rem(row, per_kv) == g), lambdas[g], factor)

    for i in range(3, 10):
        weights[i].start()

    def attend(index, carry):
        first = index * group
        for i in range(group):
            kv_copy(first + i).wait()
        stage = []
        values = []
        for i in range(group):
            pack = first + i
            keys = []
            swapped = []
            for j in range(0, side, 2):
                even = kv[side * pack + j]
                odd = pltpu.roll(kv[side * pack + j + 1], v_width, 1)
                keys += [even[:, :v_width], odd[:, v_width:]]
                swapped += [odd[:, :v_width], even[:, v_width:]]
            keys = jnp.concatenate(keys, axis=1)
            values.append(jnp.concatenate(swapped, axis=1))
            query = q_rows[pl.ds(pl.multiple_of(pack * block, block), block), :]
            stage.append(mm_t(query, keys))
        weighed = []
        for i in range(group):
            pack = first + i
            fresh = score_new[pl.ds(pl.multiple_of(pack * block, block), block), :][:, :1]
            owner = lax.rem(iota((block, 1), 0), half) // per_kv
            limit = jnp.zeros((block, 1), jnp.int32)
            for j in range(side):
                limit = jnp.where(owner == j, lengths[side * pack + j], limit)
            valid = iota((block, cache_len), 1) < limit
            scores = jnp.where(valid, stage[i], neg_fill)
            highest = jnp.maximum(jnp.max(scores, axis=1, keepdims=True), fresh)
            expo = jnp.exp((scores - highest) * scaling)
            expo_new = jnp.exp((fresh - highest) * scaling)
            scale = factor / (jnp.sum(expo, axis=1, keepdims=True) + expo_new)
            expo = expo * scale
            expo_new = expo_new * scale
            weighed.append(
                (
                    (expo[:half] - expo[half:]).astype(BF16),
                    (expo_new[:half] - expo_new[half:]).astype(BF16).astype(F32),
                )
            )
        for i in range(group):
            pack = first + i
            spots = pl.ds(pl.multiple_of(pack * half, half), half)
            mixed = mm(weighed[i][0], values[i]) + weighed[i][1] * value_new[spots, :]
            owner = iota(mixed.shape, 0) // per_kv
            own = owner + 1 - 2 * lax.rem(owner, 2) == iota(mixed.shape, 1) // v_width
            mix_rows[spots, :] = jnp.where(own, mixed, 0.0)
        return carry

    def spread_rows(source):
        rows_out = lax.dot_general(
            relay_pick[source], relay[source], (((0,), (0,)), ((), ())), preferred_element_type=F32
        )
        for q in range(plane):
            packed[source, q] = rows_out[q * capacity : (q + 1) * capacity, :].astype(BF16)
        arrived[tp, source, lo] = packed[source, spot_in_plane]
        for q in range(1, plane):
            other = lax.rem(spot_in_plane + q, plane)
            remote(
                packed.at[source, other],
                arrived.at[tp, source, lo],
                disp_sem,
                hi * n_lo + other // n_tp,
                lax.rem(other, n_tp),
            ).start()

    def open_links():
        pl.semaphore_wait(barrier, n_dev - 1)
        outer = (hi != half_planes - 1 + upper).astype(jnp.int32)
        for k in range(len(far_planes)):
            k = k + outer * (half_planes - 1 - 2 * k)
            relay_copy(hi, half_planes - upper + k * (1 - 2 * upper)).start()
        for other in near_planes:
            relay_copy(hi, other).start()
        relay[hi] = tokens[:, pl.ds(pl.multiple_of(tp * share, share), share)]
        spread_rows(hi)

    first_part = packs // group // 2
    pl.when(hi == n_hi - 1)(open_links)
    lax.fori_loop(0, first_part, attend, 0)
    pl.when((me >= 2) & (hi < n_hi - 1))(open_links)
    lax.fori_loop(first_part, packs // group, attend, 0)
    pl.when(me < 2)(open_links)

    mixed = mix_rows[...]
    mean = jnp.sum(mixed * mixed, axis=1, keepdims=True) * (1.0 / v_width)
    head_out = (mixed * lax.rsqrt(mean + epsilon) * wide_gain).astype(BF16)
    unfold = (fold_width, per_kv * v_width)
    shifted = hot(lax.rem(iota(unfold, 1), v_width) == lax.rem(iota(unfold, 0), v_width))
    laid = mm(head_out, shifted)
    own = iota(laid.shape, 1) // v_width == lax.rem(iota(laid.shape, 0), per_kv)
    laid = jnp.where(own, laid, 0.0).astype(BF16)
    gather = (seqs, seqs * per_kv)
    heads[tp] = mm(hot(iota(gather, 1) // per_kv == iota(gather, 0)), laid).astype(BF16)

    for t in range(1, n_tp):
        remote(heads.at[tp], heads.at[tp], head_sem, ep, lax.rem(tp + t, n_tp)).start()
    picked_rows = lax.dot_general(
        row_choice, laid, (((0,), (0,)), ((), ())), preferred_element_type=F32
    )
    for e in range(n_dev):
        head_rows[e] = picked_rows[e * capacity : (e + 1) * capacity, :].astype(BF16)
    head_slots[tp * n_ep + ep] = head_rows[me]
    for other_ep, other_tp in peers:
        remote(
            head_rows.at[other_ep * n_tp + other_tp],
            head_slots.at[tp * n_ep + ep],
            slot_sem,
            other_ep,
            other_tp,
        ).start()
    for source in near_planes + far_planes:
        relay_copy(source, lax.rem(hi + 1, n_hi)).wait_recv()
        spread_rows(source)
    weights[3].wait()
    whole(heads, heads, head_sem, n_tp - 1).wait_recv()
    depth = heads.shape[2]
    projected = jnp.zeros((seqs, width), F32)
    for i in range(n_tp):
        piece = mm(heads[i], wo[i * depth : (i + 1) * depth, :])
        projected = projected + piece.astype(BF16).astype(F32)
    residual = (tokens[...].astype(F32) + projected).astype(BF16).astype(F32)
    for i in range(n_tp):
        resid[i] = residual[:, i * share : (i + 1) * share]
    ffn_in = rms(residual, ffn_gain[...]).astype(BF16)

    for i in range(4, 7):
        weights[i].wait()
    shared_act = (jax.nn.silu(mm(ffn_in, sg[...])) * mm(ffn_in, su[...])).astype(BF16)
    shared_part = mm(shared_act, sd[...])
    for i in range(n_tp):
        share_out[i] = shared_part[:, i * share : (i + 1) * share].astype(BF16)

    for t in range(1, n_tp):
        other = lax.rem(tp + t, n_tp)
        remote(share_out.at[other], share_in.at[t - 1], share_sem, ep, other).start()

    whole(head_rows, head_slots, slot_sem, n_dev - 1).wait_recv()
    projected = jnp.zeros((n_ep * capacity, width), F32)
    for i in range(n_tp):
        piece = flat_slots(head_slots[i * n_ep : (i + 1) * n_ep]).astype(BF16)
        piece = mm(piece, wo[i * depth : (i + 1) * depth, :])
        projected = projected + piece.astype(BF16).astype(F32)
    relayed_all = packed.at[:, pl.ds(0, plane - 1)]
    remote(relayed_all, relayed_all, disp_sem, ep, lax.rem(tp + 1, n_tp)).wait_recv()
    for i in range(7, 10):
        weights[i].wait()
    rows_in = [
        flat_slots(arrived[i].reshape(n_ep, capacity, share)) for i in range(n_tp)
    ]
    residual = (jnp.concatenate(rows_in, axis=1) + projected).astype(BF16).astype(F32)
    flat = rms(residual, ffn_gain[...]).astype(BF16)
    act = (jax.nn.silu(mm(flat, eg[...])) * mm(flat, eu[...])).astype(BF16)
    result = mm(act, ed[...])
    for e in range(n_ep):
        for t in range(n_tp):
            computed[e * n_tp + t] = result[
                e * capacity : (e + 1) * capacity, t * share : (t + 1) * share
            ].astype(BF16)
    returned[me] = computed[me]
    rising = [k + (k >= ep).astype(jnp.int32) for k in range(n_ep - 1)]
    rising = [(other, lax.rem(tp + t, n_tp)) for other in rising for t in range(n_tp)]
    for other_ep, other_tp in rising + peers[len(rising) :]:
        remote(
            computed.at[other_ep * n_tp + other_tp], returned.at[me], back_sem, other_ep, other_tp
        ).start()
    total = resid[tp] + share_out[tp].astype(F32)
    whole(share_out, share_in, share_sem, n_tp - 1).wait_recv()
    for i in range(n_tp - 1):
        total = total + share_in[i].astype(F32)
    whole(heads, heads, head_sem, n_tp - 1).wait_send()
    whole(share_out, share_in, share_sem, n_tp - 1).wait_send()
    whole(head_rows, head_slots, slot_sem, n_dev - 1).wait_send()
    whole(relay, relay, relay_sem, n_hi - 1).wait_send()
    remote(relayed_all, relayed_all, disp_sem, ep, lax.rem(tp + 1, n_tp)).wait_send()
    whole(computed, returned, back_sem, n_dev - 1).wait_recv()
    back = flat_slots(returned[...]).astype(BF16)
    routed = mm(mix_high, back) + mm(mix_low, back)
    out[...] = (total + routed).astype(BF16)

    whole(computed, returned, back_sem, n_dev - 1).wait_send()


def shards(
    n_ep,
    n_tp,
    tokens,
    kv_cache,
    lengths,
    attn_gain,
    w_query,
    w_key,
    w_value,
    lambdas,
    head_gain,
    w_out,
    ffn_gain,
    w_shared_gate,
    w_shared_up,
    w_shared_down,
    routing,
    route_weights,
    w_exp_gate,
    w_exp_up,
    w_exp_down,
):
    seqs, width = tokens.shape
    lanes = kv_cache.shape[2]
    v_width = head_gain.shape[0]
    per_kv = lambdas.shape[0]
    n_dev = n_ep * n_tp
    capacity = max(2, 2 * seqs * routing.shape[1] // (w_exp_gate.shape[0] * n_dev))
    share = width // n_tp
    n_lo = 2 if n_ep % 2 == 0 else 1
    n_hi = n_ep // n_lo
    plane = n_lo * n_tp
    side = lanes // v_width * 2
    packs = seqs // side
    rows = seqs * per_kv
    fold = side * v_width
    group = next(g for g in (4, 2, 1) if packs % g == 0)
    small = [
        lengths,
        lambdas,
        tokens,
        attn_gain[None, :],
        head_gain[None, :],
        ffn_gain[None, :],
        routing.T,
        route_weights.T,
    ]
    big = [
        kv_cache,
        w_query,
        w_key.T,
        w_value.T,
        w_out,
        w_shared_gate,
        w_shared_up,
        w_shared_down,
        w_exp_gate,
        w_exp_up,
        w_exp_down,
    ]
    held = [pltpu.SMEM(x.shape, x.dtype) for x in small[:2]]
    held += [pltpu.VMEM(x.shape, x.dtype) for x in small[2:]]
    held += [pltpu.VMEM(x.shape, BF16) for x in big[:8]]
    held += [pltpu.VMEM(x.shape[1:], BF16) for x in big[8:]]
    vmem = pl.BlockSpec(memory_space=pltpu.VMEM)
    dma = pltpu.SemaphoreType.DMA
    return pl.pallas_call(
        functools.partial(layer, n_ep, n_tp, capacity, group),
        out_shape=pltpu.VMEM((seqs, share), BF16),
        in_specs=[pl.BlockSpec(memory_space=pltpu.HBM)] * (len(small) + len(big)),
        out_specs=vmem,
        scratch_shapes=held
        + [
            pltpu.VMEM((2 * rows, fold), BF16),
            pltpu.VMEM((2 * rows, lanes), F32),
            pltpu.VMEM((rows, fold), F32),
            pltpu.VMEM((rows, fold), F32),
            pltpu.VMEM((n_tp, seqs, per_kv * v_width), BF16),
            pltpu.VMEM((n_dev, capacity, per_kv * v_width), BF16),
            pltpu.VMEM((n_dev, capacity, per_kv * v_width), BF16),
            pltpu.VMEM((n_tp, seqs, share), F32),
            pltpu.VMEM((n_hi, seqs, plane * capacity), BF16),
            pltpu.VMEM((n_hi, seqs, share), BF16),
            pltpu.VMEM((n_hi, plane, capacity, share), BF16),
            pltpu.VMEM((n_tp, n_hi, n_lo, capacity, share), BF16),
            pltpu.VMEM((n_dev, capacity, share), BF16),
            pltpu.VMEM((n_dev, capacity, share), BF16),
            pltpu.VMEM((n_tp, seqs, share), BF16),
            pltpu.VMEM((n_tp, seqs, share), BF16),
            dma((len(small),)),
            dma((packs,)),
            dma((10,)),
            dma((2,)),
            dma((2,)),
            dma((1 + n_hi,)),
            dma((2,)),
            dma((2,)),
            dma((2,)),
        ],
        compiler_params=pltpu.CompilerParams(
            collective_id=0, has_side_effects=True, vmem_limit_bytes=60 * 1024 * 1024
        ),
    )(
        *small,
        *big,
    )


def solution(mesh):
    return jax.shard_map(
        functools.partial(shards, mesh.shape["ep"], mesh.shape["tp"]),
        mesh=mesh,
        in_specs=(
            P("ep", None),
            P("ep", None, "tp"),
            P("ep"),
            P(),
            P(None, "tp"),
            P(None, "tp"),
            P(None, "tp"),
            P("tp"),
            P(),
            P(),
            P(),
            P(None, "tp"),
            P(None, "tp"),
            P("tp", None),
            P(),
            P("ep", None),
            P(("ep", "tp"), None, None),
            P(("ep", "tp"), None, None),
            P(("ep", "tp"), None, None),
        ),
        out_specs=P("ep", "tp"),
        check_vma=False,
    )
```
